256 devices in a mesh: ep: 64 (over z, y, core), tp: 4 (over x).
Axes of the slice: x: 4, y: 4, z: 8, core: 2. Of those that a mesh axis runs over, the one named last changes fastest.
Arguments:
- query: bfloat16 [8192, 1536], P('ep', 'tp'), may hold values from -136 to 136
- latent: bfloat16 [8192, 512], P(('ep', 'tp')), may hold values from -6 to 6
- rope_key: bfloat16 [8192, 32], P(('ep', 'tp')), may hold values from -6 to 6
- latent_gain: float32 [512], replicated, may hold values from 0.1 to 1.9
- key_up: bfloat16 [512, 1024], P(None, 'tp'), may hold values from -0.25 to 0.25
- value_up: bfloat16 [512, 1024], P(None, 'tp'), may hold values from -2 to 2
- out_proj: bfloat16 [1024, 2048], replicated, may hold values from -0.1875 to 0.1875
- tokens: bfloat16 [16384, 2048], P(('ep', 'tp')), may hold values from -6 to 6
- moe_gain: float32 [2048], replicated, may hold values from 0.1 to 1.9
- routes: int32 [16384, 2], P(('ep', 'tp')), may hold values from 0 to 63, all different within a row; in each aligned block of 64 rows (0 to 63, 64 to 127, ...) at most 4 rows name the same one
- group_prob: float32 [16384], P(('ep', 'tp')), may hold values from 0.25 to 1
- expert_prob: float32 [16384, 2], P(('ep', 'tp')), may hold values from 0.02 to 1
- w_gate: bfloat16 [64, 2048, 1024], P('ep', None, 'tp'), may hold values from -0.125 to 0.125
- w_up: bfloat16 [64, 2048, 1024], P('ep', None, 'tp'), may hold values from -0.125 to 0.125
- w_down: bfloat16 [64, 1024, 2048], P('ep', 'tp'), may hold values from -0.1875 to 0.1875
Outputs:
- mixed: bfloat16 [8192, 2048], P(('ep', 'tp'))
- moe_out: bfloat16 [16384, 2048], P(('ep', 'tp'))
The draws below stay inside these ranges and needn't reach their ends.
Inputs may be any that keep to these rules, and one draw needn't show every extreme that they name: `routes`: each row names 2 different experts; within the rows of one device no expert is named more than 4 times.
All inputs are finite; a program needn't handle non-finite values.
Results may differ from the reference program's by a relative error of at most 0.025.
Values may be sent and summed in bfloat16 or wider, within the bound.
A program may use at most 128 MiB of HBM per device.

```python
import functools
import math
import jax
import jax.numpy as jnp
import numpy as np
from jax import lax

D = 2048
HEADS = 16
NOPE = 64
ROPE_DIM = 32
V_DIM = 64
LATENT = 512
EXPERT_WIDTH = 1024
TOP = 2
M_ROWS = 64
SEQ = 8192
MOE_TOKENS = 16384
EXPERTS = 64
CAP = 4
N_TP = 4


def draw_query(key, part):
    first_key = jax.random.fold_in(jax.random.fold_in(key, 11), 0)
    full_shape = (SEQ, HEADS * (NOPE + ROPE_DIM))
    values = jnp.clip(2.0 * jax.random.normal(first_key, full_shape, jnp.float32), -8.0, 8.0)
    return values.astype(jnp.bfloat16)


def block_scale(own_key, dims, cuts, smallest, top_value):
    def one(position, blocks):
        draws = jax.random.uniform(jax.random.fold_in(jax.random.fold_in(own_key, 6), position), (blocks,), jnp.float32, smallest / len(cuts), top_value / len(cuts))
        return jnp.repeat(jnp.exp(draws), dims[position] // blocks).reshape((-1,) + (1,) * (len(dims) - position - 1))

    factor_of = one(*cuts[0])
    for cut in cuts[1:]:
        factor_of = factor_of * one(*cut)
    return factor_of


def assign_block(stream_key, own, number, rows, count, top, most, slope):
    order = jax.random.permutation(stream_key, count)
    crowded, usual = portions_of(count, rows * top, most, slope, True), portions_of(count, rows * top, most, slope, False)
    places = jnp.arange(count)

    def named(lengths, turn):
        used = int((lengths > 0).sum())
        fixed = max(1, used // 4)
        shifted = fixed + (places - fixed + turn * (used - fixed)) % max(1, count - fixed)
        return jnp.zeros((count,), jnp.int32).at[order[jnp.where(places < fixed, places, shifted)]].set(jnp.asarray(lengths, jnp.int32))

    lengths = jnp.where(number % 4 == 0, named(crowded, number // 4), named(usual, number - number // 4 - 1))
    mixed = jax.random.permutation(jax.random.fold_in(own, 3), count)
    source_of, taker = mixed[0:count // 2 * 2:2], mixed[1:count // 2 * 2:2]
    room = jnp.minimum(lengths[source_of] - 1, most - lengths[taker]) // 2
    room = jnp.where((source_of == order[0]) | (taker == order[0]) | (lengths[taker] == 0), 0, jnp.maximum(room, 0))
    shifted = jax.random.randint(jax.random.fold_in(own, 4), (count // 2,), 0, 1 << 20) % (room + 1)
    lengths = lengths.at[source_of].add(-shifted).at[taker].add(shifted)
    items = jnp.searchsorted(jnp.cumsum(lengths), jnp.arange(rows * top), side="right").astype(jnp.int32)
    grid = items.reshape(top, rows).T
    grid = grid[jax.random.permutation(jax.random.fold_in(own, 1), rows)]
    turn = jax.random.randint(jax.random.fold_in(own, 2), (rows, 1), 0, top)
    return jnp.take_along_axis(grid, (jnp.arange(top)[None, :] + turn) % top, axis=1)


def portions_of(number_of, total, reach, slope, full):
    portions = [(1 << 20) // math.isqrt(standing ** slope) + 1 for standing in range(1, number_of + 1)]
    largest = reach if full else min(reach, max(-(-total // number_of), total * portions[0] // sum(portions)))
    least = 1 if total - largest >= number_of - 1 else 0
    given, rest = [largest] + [least] * (number_of - 1), total - largest - least * (number_of - 1)
    while rest > 0:
        movable = [i for i in range(1, number_of) if given[i] < largest] or [i for i in range(1, number_of) if given[i] < reach]
        pool, budget = sum([portions[i] for i in movable]), rest
        for i in movable:
            more = min(reach - given[i], max(1, budget * portions[i] // pool), rest)
            given[i] = given[i] + more
            rest = rest - more
    return np.array(given)


def centred(key, shape, spread, bound, cuts=(), kind=jnp.bfloat16):
    array = jax.random.normal(key, shape, jnp.float32) * spread
    if len(cuts) > 0:
        array = block_scale(key, shape, cuts, -0.22, 0.18) * array
    return jnp.clip(array, min=-bound, max=bound).astype(kind)


def setup_inputs(seed: int = 0) -> dict:
    key_list = jax.random.split(jax.random.key(seed), 16)
    query = draw_query(jax.random.fold_in(key_list[15], 71), 0)
    latent = centred(key_list[1], (SEQ, LATENT), 1.0, 6.0, ((0, 256),))
    rope_key = centred(key_list[2], (SEQ, ROPE_DIM), 1.0, 6.0, ((0, 256),))
    latent_gain = jnp.clip(1.0 + 0.18 * jax.random.normal(key_list[3], (LATENT,), jnp.float32), 0.1, 1.9)
    key_up = centred(key_list[4], (LATENT, HEADS * NOPE), LATENT ** -0.5, 0.25, ((1, 4),))
    value_up = centred(key_list[5], (LATENT, HEADS * V_DIM), (LATENT // 64) ** -0.5, 2.0, ((1, 4),))
    out_proj = centred(key_list[6], (HEADS * V_DIM, D), (HEADS * V_DIM) ** -0.5, 0.1875)
    tokens = centred(key_list[7], (MOE_TOKENS, D), 1.0, 6.0, ((0, 256),))
    moe_gain = jnp.clip(1.0 + 0.18 * jax.random.normal(key_list[8], (D,), jnp.float32), 0.1, 1.9)
    routes_keys = jax.random.split(jax.random.fold_in(key_list[9], 1), MOE_TOKENS // M_ROWS)
    routes_turns = jax.random.permutation(jax.random.fold_in(key_list[9], 3), MOE_TOKENS // M_ROWS)
    routes = jax.vmap(lambda own, number: assign_block(jax.random.fold_in(key_list[9], 2), own, number, M_ROWS, EXPERTS, TOP, CAP, 2))(routes_keys, routes_turns).reshape((MOE_TOKENS, TOP))
    group_prob = jnp.clip(jnp.exp(math.log(1.0) - 1.3862944 * jax.random.uniform(key_list[10], (MOE_TOKENS,), jnp.float32) ** block_scale(key_list[10], (MOE_TOKENS,), ((0, 256),), -0.2, 0.2)), 0.25, 1.0)
    expert_prob = jnp.clip(jnp.exp(math.log(1.0) - 3.912023 * jax.random.uniform(key_list[11], (MOE_TOKENS, TOP), jnp.float32) ** block_scale(key_list[11], (MOE_TOKENS, TOP), ((0, 256),), -0.2, 0.2)), 0.02, 1.0)
    w_gate = centred(key_list[12], (EXPERTS, D, EXPERT_WIDTH), D ** -0.5, 0.125, ((0, 64), (2, 4)))
    w_up = centred(key_list[13], (EXPERTS, D, EXPERT_WIDTH), D ** -0.5, 0.125, ((0, 64), (2, 4)))
    w_down = centred(key_list[14], (EXPERTS, EXPERT_WIDTH, D), EXPERT_WIDTH ** -0.5, 0.1875, ((0, 64), (1, 4)))
    return {"query": query, "latent": latent, "rope_key": rope_key, "latent_gain": latent_gain, "key_up": key_up, "value_up": value_up, "out_proj": out_proj, "tokens": tokens, "moe_gain": moe_gain, "routes": routes, "group_prob": group_prob, "expert_prob": expert_prob, "w_gate": w_gate, "w_up": w_up, "w_down": w_down}


epsilon = 1e-06
rope_base = 10000.0
masked_value = -1e+30

def rms_scale(values, gain):
    widened = values.astype(jnp.float32)
    return widened * lax.rsqrt(lax.optimization_barrier(jnp.mean(widened * widened, axis=-1, keepdims=True)) + epsilon) * gain.astype(jnp.float32)

def tables(positions, rope_width):
    half_width = rope_width // 2
    inverse = rope_base ** (-2.0 * jnp.arange(half_width, dtype=jnp.float32) / rope_width)
    angles = positions.astype(jnp.float32)[:, None] * inverse[None, :]
    return (jnp.cos(angles), jnp.sin(angles))

def rotate(values, cosine, sine):
    half_width = values.shape[-1] // 2
    lower = values[..., :half_width]
    upper = values[..., half_width:]
    return jnp.concatenate([lower * cosine - upper * sine, lower * sine + upper * cosine], axis=-1)

def head_attention(rope_prefix, query_pos, parts):
    query_head, key_head, value_head = parts
    full_keys = jnp.concatenate([key_head, rope_prefix], axis=-1)
    scores = jnp.dot(query_head, full_keys.T, preferred_element_type=jnp.float32) * (NOPE + ROPE_DIM) ** (-0.5)
    key_pos = jnp.arange(full_keys.shape[0], dtype=jnp.int32)
    allowed = key_pos[None, :] <= query_pos[:, None]
    scores = jnp.where(allowed, scores, masked_value)
    row_peak = lax.optimization_barrier(jnp.max(scores, axis=-1, keepdims=True))
    raised = jnp.where(allowed, jnp.exp(scores - row_peak), 0.0)
    totals = lax.optimization_barrier(jnp.sum(raised, axis=-1, keepdims=True))
    summed = jnp.dot(raised.astype(jnp.bfloat16), value_head, preferred_element_type=jnp.float32)
    return (summed / totals).astype(jnp.bfloat16)

def mixer_reference(query, latent, rope_key, latent_gain, key_up, value_up, out_proj):
    seq_len = latent.shape[0]
    positions = jnp.arange(seq_len, dtype=jnp.int32)
    cosine, sine = tables(positions, ROPE_DIM)
    normed = rms_scale(latent, latent_gain).astype(jnp.bfloat16)
    rotated_key = rotate(rope_key.astype(jnp.float32), cosine, sine).astype(jnp.bfloat16)
    query_heads = query.reshape(seq_len, HEADS, NOPE + ROPE_DIM)
    turned = rotate(query_heads[..., NOPE:].astype(jnp.float32), cosine[:, None, :], sine[:, None, :]).astype(jnp.bfloat16)
    rotated_query = jnp.concatenate([query_heads[..., :NOPE], turned], axis=-1)
    key_nope = jnp.dot(normed, key_up, preferred_element_type=jnp.float32).astype(jnp.bfloat16).reshape(seq_len, HEADS, NOPE)
    values = jnp.dot(normed, value_up, preferred_element_type=jnp.float32).astype(jnp.bfloat16).reshape(seq_len, HEADS, V_DIM)
    block_len = math.gcd(seq_len, 512)
    pieces = []
    for block_at in range(seq_len // block_len):
        upto = (block_at + 1) * block_len
        query_pos = positions[block_at * block_len:upto]
        parts = (rotated_query[block_at * block_len:upto].transpose(1, 0, 2), key_nope[:upto].transpose(1, 0, 2), values[:upto].transpose(1, 0, 2))
        result = lax.map(functools.partial(head_attention, rotated_key[:upto], query_pos), parts)
        pieces.append(result.transpose(1, 0, 2).reshape(block_len, HEADS * V_DIM))
    attention = jnp.concatenate(pieces, axis=0)
    return jnp.dot(attention, out_proj, preferred_element_type=jnp.float32).astype(jnp.bfloat16)

def expert_reference(tokens, moe_gain, routes, group_prob, expert_prob, w_gate, w_up, w_down):
    amount = tokens.shape[0]
    model_width = tokens.shape[1]
    expert_count = w_gate.shape[0]
    block_count = amount // M_ROWS
    normed = rms_scale(tokens, moe_gain).astype(jnp.bfloat16)
    flat_routes = routes.reshape(block_count, M_ROWS * TOP)
    onehot = (flat_routes[:, :, None] == jnp.arange(expert_count, dtype=jnp.int32)[None, None, :]).astype(jnp.int32)
    earlier = jnp.cumsum(onehot, axis=1) - onehot
    slot_index = lax.optimization_barrier(jnp.sum(earlier * onehot, axis=2))
    block_ids = jnp.arange(block_count, dtype=jnp.int32)[:, None]
    place = block_ids * CAP + slot_index
    source_row = block_ids * M_ROWS + jnp.arange(M_ROWS * TOP, dtype=jnp.int32)[None, :] // TOP
    shares = group_prob[:, None] * expert_prob / lax.optimization_barrier(jnp.sum(expert_prob, axis=1, keepdims=True))
    row_table = jnp.full((expert_count, block_count * CAP), amount, jnp.int32).at[flat_routes, place].set(source_row)
    share_table = jnp.zeros((expert_count, block_count * CAP), jnp.float32).at[flat_routes, place].set(shares.reshape(block_count, M_ROWS * TOP))
    padded = jnp.concatenate([normed, jnp.zeros((1, model_width), jnp.bfloat16)], axis=0)
    group_width = w_down.shape[1] // N_TP

    def per_expert(running, parts):
        row_ids, row_shares, gate_weight, up_weight, down_weight = parts
        rows_here = padded[row_ids]
        gate_values = jnp.dot(rows_here, gate_weight, preferred_element_type=jnp.float32)
        up_values = jnp.dot(rows_here, up_weight, preferred_element_type=jnp.float32)
        hidden = (jax.nn.silu(gate_values) * up_values).astype(jnp.bfloat16)
        summed = jnp.zeros((rows_here.shape[0], model_width), jnp.float32)
        for group_at in range(N_TP):
            lower_edge = group_at * group_width
            partial_low = jnp.dot(hidden[:, lower_edge:lower_edge + group_width], down_weight[lower_edge:lower_edge + group_width], preferred_element_type=jnp.float32).astype(jnp.bfloat16)
            partial_low = lax.optimization_barrier(partial_low)
            summed = summed + partial_low.astype(jnp.float32)
        expert_out = summed.astype(jnp.bfloat16)
        expert_out = lax.optimization_barrier(expert_out)
        running = running.at[row_ids].add(row_shares[:, None] * expert_out.astype(jnp.float32))
        return (running, None)
    running, _ = lax.scan(per_expert, jnp.zeros((amount + 1, model_width), jnp.float32), (row_table, share_table, w_gate, w_up, w_down))
    return running[:amount].astype(jnp.bfloat16)

def reference(query, latent, rope_key, latent_gain, key_up, value_up, out_proj, tokens, moe_gain, routes, group_prob, expert_prob, w_gate, w_up, w_down):
    mixed = mixer_reference(query, latent, rope_key, latent_gain, key_up, value_up, out_proj)
    moe_out = expert_reference(tokens, moe_gain, routes, group_prob, expert_prob, w_gate, w_up, w_down)
    return (mixed, moe_out)
```

```python
import math

import jax
import jax.numpy as jnp
from jax import lax
from jax.experimental import pallas as pl
from jax.experimental.pallas import tpu as pltpu
from jax.sharding import PartitionSpec as P

NOPE = 64
ROPE_DIM = 32
V_DIM = 64
GROUP = 8


epsilon = 1e-06
rope_base = 10000.0
masked_value = -1e30


def in_one_piece(arrays, axis, dim, along):
    both = jnp.concatenate(arrays, axis=along)
    out, at, done = (lax.all_gather(both, axis, axis=dim, tiled=True), 0, [])
    for a in arrays:
        done.append(lax.slice_in_dim(out, at, at + a.shape[along], axis=along))
        at += a.shape[along]
    return tuple(done)


def split_up(value, dim, devices):
    before, after = (value.shape[:dim], value.shape[dim + 1 :])
    return jnp.moveaxis(value.reshape(*before, devices, -1, *after), dim, 0)


def sent_and_summed(value, axis, dim):
    devices = lax.axis_size(axis)
    parts = lax.all_to_all(split_up(value, dim, devices), axis, 0, 0, tiled=True)
    return jnp.sum(parts.astype(jnp.float32), axis=0)


def rms_scale(values, gain):
    widened = values.astype(jnp.float32)
    return widened * lax.rsqrt(jnp.mean(widened * widened, axis=-1, keepdims=True) + epsilon) * gain


def tables(positions, rope_width):
    half_width = rope_width // 2
    inverse = rope_base ** (-2.0 * jnp.arange(half_width, dtype=jnp.float32) / rope_width)
    angles = positions.astype(jnp.float32)[:, None] * inverse[None, :]
    return (jnp.cos(angles), jnp.sin(angles))


def rotate(values, cosine, sine):
    half_width = values.shape[-1] // 2
    lower = values[..., :half_width]
    upper = values[..., half_width:]
    return jnp.concatenate([lower * cosine - upper * sine, lower * sine + upper * cosine], axis=-1)


def attend(queries, kv):
    ranks = kv.shape[0]
    groups = ranks // GROUP
    shift = math.log2(math.e) / math.sqrt(NOPE + ROPE_DIM)

    def kernel(q_ref, kv_ref, o_ref, held, sem):
        me = lax.axis_index("ep")
        last = me // GROUP

        def fetch(g):
            return pltpu.make_async_copy(
                kv_ref.at[pl.ds(g * GROUP, GROUP)], held.at[pl.ds(g * GROUP, GROUP)], sem.at[g]
            )

        for g in range(groups):

            @pl.when(g <= last)
            def _():
                fetch(g).start()

        def step(g, state, masked):
            fetch(g).wait()
            out = []
            base = g * GROUP
            rope = held[pl.ds(base, GROUP), 512:544, :].reshape(GROUP * 32, 128)
            for p in range(2):
                top, total, acc = state[p]
                parts = []
                for j in range(4):
                    keys = held[pl.ds(base, GROUP), 128 * p + 32 * j : 128 * p + 32 * j + 32, :]
                    both = jnp.concatenate([keys.reshape(GROUP * 32, 128), rope], axis=1)
                    s = lax.dot_general(
                        both, q_ref[p, j], (((1,), (1,)), ((), ())), preferred_element_type=jnp.float32
                    )
                    s = s.reshape(GROUP, 32, 256)
                    if masked:
                        rank = lax.broadcasted_iota(jnp.int32, s.shape, 0) + base
                        row = lax.broadcasted_iota(jnp.int32, s.shape, 1) + 32 * j
                        col = lax.broadcasted_iota(jnp.int32, s.shape, 2) & 127
                        s = jnp.where(rank * 128 + row <= me * 128 + col, s, masked_value)
                    parts.append(s)
                peak = parts[0].max(axis=0)
                for s in parts[1:]:
                    peak = jnp.maximum(peak, s.max(axis=0))
                peak = jnp.maximum(top, peak.max(axis=0, keepdims=True))
                factor = jnp.exp2((top - peak) * shift)
                summed = jnp.zeros((32, 256), jnp.float32)
                raised = []
                for s in parts:
                    r = jnp.exp2((s - peak[None]) * shift)
                    summed = summed + r.sum(axis=0)
                    raised.append(r.astype(jnp.bfloat16))
                total = total * factor + summed.sum(axis=0, keepdims=True)
                acc = acc * factor
                weights = jnp.concatenate(raised, axis=1)
                for r in range(0, GROUP, 2):
                    vals = jnp.concatenate(
                        [held[base + r + i, 256 + 128 * p : 384 + 128 * p, :] for i in range(2)], axis=1
                    )
                    acc = acc + jnp.dot(
                        vals, weights[r : r + 2].reshape(256, 256), preferred_element_type=jnp.float32
                    )
                out.append((peak, total, acc))
            return tuple(out)

        start = tuple(
            (
                jnp.full((1, 256), masked_value, jnp.float32),
                jnp.zeros((1, 256), jnp.float32),
                jnp.zeros((128, 256), jnp.float32),
            )
            for _ in range(2)
        )
        state = lax.fori_loop(0, last, lambda g, s: step(g, s, False), start)
        state = step(last, state, True)
        pieces = []
        for p in range(2):
            _, total, acc = state[p]
            for i in range(2):
                pieces.append(acc[64 * i : 64 * i + 64, 128 * i : 128 * i + 128] / total[:, 128 * i : 128 * i + 128])
        o_ref[...] = jnp.concatenate(pieces, axis=0).T.astype(jnp.bfloat16)

    return pl.pallas_call(
        kernel,
        out_shape=jax.ShapeDtypeStruct((128, 256), jnp.bfloat16),
        in_specs=[pl.BlockSpec(memory_space=pltpu.VMEM), pl.BlockSpec(memory_space=pl.ANY)],
        out_specs=pl.BlockSpec(memory_space=pltpu.VMEM),
        scratch_shapes=[pltpu.VMEM(kv.shape, jnp.bfloat16), pltpu.SemaphoreType.DMA((groups,))],
        compiler_params=pltpu.CompilerParams(vmem_limit_bytes=40 << 20),
        name="attend",
    )(queries, kv)


def query_rows(query, positions):
    rows = query.shape[0]
    cosine, sine = tables(positions, ROPE_DIM)
    heads = query.reshape(rows, 4, NOPE + ROPE_DIM)
    turned = rotate(heads[..., NOPE:].astype(jnp.float32), cosine[:, None, :], sine[:, None, :])
    turned = turned.astype(jnp.bfloat16).transpose(1, 0, 2)
    flat = heads[..., :NOPE].transpose(1, 0, 2)
    out = []
    for p in range(2):
        for j in range(4):
            for i in range(2):
                h = 2 * p + i
                nope = jnp.pad(flat[h], ((0, 0), (64 * i, 64 - 64 * i)))
                rope = jnp.pad(turned[h], ((0, 0), (32 * j, 96 - 32 * j)))
                out.append(jnp.concatenate([nope, rope], axis=1))
    return jnp.stack(out).reshape(2, 4, 256, 256)


def mixer_half(query, latent, rope_key, latent_gain, key_up, value_up, out_proj):
    rows = query.shape[0]
    own_rows = latent.shape[0]
    query_start = lax.axis_index("ep") * rows
    key_start = query_start + lax.axis_index("tp") * own_rows
    normed = rms_scale(latent, latent_gain).astype(jnp.bfloat16)
    key_cos, key_sin = tables(key_start + jnp.arange(own_rows, dtype=jnp.int32), ROPE_DIM)
    rotated_key = rotate(rope_key.astype(jnp.float32), key_cos, key_sin).astype(jnp.bfloat16)
    queries = query_rows(query, query_start + jnp.arange(rows, dtype=jnp.int32))
    group_latent, group_rope = in_one_piece((normed, rotated_key), "tp", 0, 1)
    keys = jnp.dot(group_latent, key_up, preferred_element_type=jnp.float32).astype(jnp.bfloat16)
    values = lax.dot_general(
        value_up, group_latent, (((0,), (1,)), ((), ())), preferred_element_type=jnp.float32
    ).astype(jnp.bfloat16)
    rope = group_rope.reshape(4, 32, 32).transpose(1, 0, 2).reshape(32, 128)
    kv = jnp.concatenate([keys[:, :128], keys[:, 128:], values, rope], axis=0)
    kv = lax.all_gather(kv, "ep", axis=0)
    attention = attend(queries, kv)
    own_attention = lax.all_to_all(attention, "tp", split_axis=0, concat_axis=1, tiled=True)
    return jnp.dot(own_attention, out_proj, preferred_element_type=jnp.float32).astype(jnp.bfloat16)


def expert_half(tokens, moe_gain, routes, group_prob, expert_prob, w_gate, w_up, w_down):
    row_count, model_width = tokens.shape
    top_count = routes.shape[1]
    expert_count = lax.axis_size("ep")
    capacity = 2 * top_count * row_count // expert_count
    normed = rms_scale(tokens, moe_gain).astype(jnp.bfloat16)
    flat_routes = routes.reshape(-1)
    onehot = (flat_routes[:, None] == jnp.arange(expert_count, dtype=jnp.int32)[None, :]).astype(
        jnp.int32
    )
    earlier = jnp.cumsum(onehot, axis=0) - onehot
    slot_index = jnp.sum(earlier * onehot, axis=1)
    target = flat_routes * capacity + slot_index
    owner = target[None, :] == jnp.arange(expert_count * capacity, dtype=jnp.int32)[:, None]
    dispatch_table = jnp.any(
        owner.reshape(expert_count * capacity, row_count, top_count), axis=2
    ).astype(jnp.bfloat16)
    outgoing = jnp.dot(dispatch_table, normed, preferred_element_type=jnp.float32).astype(
        jnp.bfloat16
    )
    outgoing = outgoing.reshape(expert_count, capacity, model_width)
    arrived = lax.all_to_all(outgoing, "ep", split_axis=0, concat_axis=0, tiled=True)
    sources, slots, _ = arrived.shape
    flat_rows = arrived.reshape(sources * slots, model_width)
    shard_rows = lax.all_gather(flat_rows, "tp", axis=0, tiled=True)
    gate_values = jnp.dot(shard_rows, w_gate[0], preferred_element_type=jnp.float32)
    up_values = jnp.dot(shard_rows, w_up[0], preferred_element_type=jnp.float32)
    hidden = (jax.nn.silu(gate_values) * up_values).astype(jnp.bfloat16)

    def lower(offset, amount):
        return jnp.dot(hidden, w_down[0], preferred_element_type=jnp.float32)

    summed = sent_and_summed(
        lower(jnp.int32(0), sources * slots * lax.axis_size("tp")).astype(jnp.bfloat16), "tp", 0
    )
    result = summed.astype(jnp.bfloat16).reshape(sources, slots, model_width)
    returned = lax.all_to_all(result, "ep", split_axis=0, concat_axis=0, tiled=True)
    returned_flat = returned.reshape(expert_count * capacity, model_width)
    picked = returned_flat[target].reshape(row_count, top_count, model_width).astype(jnp.float32)
    shares = group_prob[:, None] * expert_prob / jnp.sum(expert_prob, axis=1, keepdims=True)
    return jnp.sum(shares[:, :, None] * picked, axis=1).astype(jnp.bfloat16)


def body(
    query,
    latent,
    rope_key,
    latent_gain,
    key_up,
    value_up,
    out_proj,
    tokens,
    moe_gain,
    routes,
    group_prob,
    expert_prob,
    w_gate,
    w_up,
    w_down,
):
    mixed = mixer_half(query, latent, rope_key, latent_gain, key_up, value_up, out_proj)
    moe_out = expert_half(tokens, moe_gain, routes, group_prob, expert_prob, w_gate, w_up, w_down)
    return (mixed, moe_out)


def solution(mesh):
    return jax.shard_map(
        body,
        mesh=mesh,
        in_specs=(
            P("ep", "tp"),
            P(("ep", "tp"), None),
            P(("ep", "tp"), None),
            P(),
            P(None, "tp"),
            P(None, "tp"),
            P(),
            P(("ep", "tp"), None),
            P(),
            P(("ep", "tp"), None),
            P(("ep", "tp")),
            P(("ep", "tp"), None),
            P("ep", None, "tp"),
            P("ep", None, "tp"),
            P("ep", "tp", None),
        ),
        out_specs=(P(("ep", "tp"), None), P(("ep", "tp"), None)),
        check_vma=False,
    )
```

```python
import math

import jax
import jax.numpy as jnp
from jax import lax
from jax.experimental import pallas as pl
from jax.experimental.pallas import tpu as pltpu
from jax.sharding import PartitionSpec as P

NOPE = 64
ROPE_DIM = 32
V_DIM = 64
GROUP = 8
MESH = pl.DeviceIdType.MESH


epsilon = 1e-06
rope_base = 10000.0
masked_value = -1e30


def in_one_piece(arrays, axis, dim, along):
    both = jnp.concatenate(arrays, axis=along)
    out, at, done = (lax.all_gather(both, axis, axis=dim, tiled=True), 0, [])
    for a in arrays:
        done.append(lax.slice_in_dim(out, at, at + a.shape[along], axis=along))
        at += a.shape[along]
    return tuple(done)


def split_up(value, dim, devices):
    before, after = (value.shape[:dim], value.shape[dim + 1 :])
    return jnp.moveaxis(value.reshape(*before, devices, -1, *after), dim, 0)


def sent_and_summed(value, axis, dim):
    devices = lax.axis_size(axis)
    parts = lax.all_to_all(split_up(value, dim, devices), axis, 0, 0, tiled=True)
    return jnp.sum(parts.astype(jnp.float32), axis=0)


def rms_scale(values, gain):
    widened = values.astype(jnp.float32)
    return widened * lax.rsqrt(jnp.mean(widened * widened, axis=-1, keepdims=True) + epsilon) * gain


def tables(positions, rope_width):
    half_width = rope_width // 2
    inverse = rope_base ** (-2.0 * jnp.arange(half_width, dtype=jnp.float32) / rope_width)
    angles = positions.astype(jnp.float32)[:, None] * inverse[None, :]
    return (jnp.cos(angles), jnp.sin(angles))


def rotate(values, cosine, sine):
    half_width = values.shape[-1] // 2
    lower = values[..., :half_width]
    upper = values[..., half_width:]
    return jnp.concatenate([lower * cosine - upper * sine, lower * sine + upper * cosine], axis=-1)


def attend(queries, kv):
    ranks = kv.shape[0]
    groups = ranks // GROUP
    shift = math.log2(math.e) / math.sqrt(NOPE + ROPE_DIM)

    def kernel(q_ref, kv_ref, o_ref, held, sem):
        me = lax.axis_index("ep")
        last = me // GROUP

        def fetch(g):
            return pltpu.make_async_copy(
                kv_ref.at[pl.ds(g * GROUP, GROUP)], held.at[pl.ds(g * GROUP, GROUP)], sem.at[g]
            )

        for g in range(groups):

            @pl.when(g <= last)
            def _():
                fetch(g).start()

        def step(g, state, masked):
            fetch(g).wait()
            out = []
            base = g * GROUP
            rope = held[pl.ds(base, GROUP), 512:544, :].reshape(GROUP * 32, 128)
            for p in range(2):
                top, total, acc = state[p]
                parts = []
                for j in range(4):
                    keys = held[pl.ds(base, GROUP), 128 * p + 32 * j : 128 * p + 32 * j + 32, :]
                    both = jnp.concatenate([keys.reshape(GROUP * 32, 128), rope], axis=1)
                    s = lax.dot_general(
                        both, q_ref[p, j], (((1,), (1,)), ((), ())), preferred_element_type=jnp.float32
                    )
                    s = s.reshape(GROUP, 32, 256)
                    if masked:
                        rank = lax.broadcasted_iota(jnp.int32, s.shape, 0) + base
                        row = lax.broadcasted_iota(jnp.int32, s.shape, 1) + 32 * j
                        col = lax.broadcasted_iota(jnp.int32, s.shape, 2) & 127
                        s = jnp.where(rank * 128 + row <= me * 128 + col, s, masked_value)
                    parts.append(s)
                peak = parts[0].max(axis=0)
                for s in parts[1:]:
                    peak = jnp.maximum(peak, s.max(axis=0))
                peak = jnp.maximum(top, peak.max(axis=0, keepdims=True))
                factor = jnp.exp2((top - peak) * shift)
                summed = jnp.zeros((32, 256), jnp.float32)
                raised = []
                for s in parts:
                    r = jnp.exp2((s - peak[None]) * shift)
                    summed = summed + r.sum(axis=0)
                    raised.append(r.astype(jnp.bfloat16))
                total = total * factor + summed.sum(axis=0, keepdims=True)
                acc = acc * factor
                weights = jnp.concatenate(raised, axis=1)
                for r in range(0, GROUP, 2):
                    vals = jnp.concatenate(
                        [held[base + r + i, 256 + 128 * p : 384 + 128 * p, :] for i in range(2)], axis=1
                    )
                    acc = acc + jnp.dot(
                        vals, weights[r : r + 2].reshape(256, 256), preferred_element_type=jnp.float32
                    )
                out.append((peak, total, acc))
            return tuple(out)

        start = tuple(
            (
                jnp.full((1, 256), masked_value, jnp.float32),
                jnp.zeros((1, 256), jnp.float32),
                jnp.zeros((128, 256), jnp.float32),
            )
            for _ in range(2)
        )
        state = lax.fori_loop(0, last, lambda g, s: step(g, s, False), start)
        state = step(last, state, True)
        pieces = []
        for p in range(2):
            _, total, acc = state[p]
            for i in range(2):
                pieces.append(acc[64 * i : 64 * i + 64, 128 * i : 128 * i + 128] / total[:, 128 * i : 128 * i + 128])
        o_ref[...] = jnp.concatenate(pieces, axis=0).T.astype(jnp.bfloat16)

    return pl.pallas_call(
        kernel,
        out_shape=jax.ShapeDtypeStruct((128, 256), jnp.bfloat16),
        in_specs=[pl.BlockSpec(memory_space=pltpu.VMEM), pl.BlockSpec(memory_space=pl.ANY)],
        out_specs=pl.BlockSpec(memory_space=pltpu.VMEM),
        scratch_shapes=[pltpu.VMEM(kv.shape, jnp.bfloat16), pltpu.SemaphoreType.DMA((groups,))],
        compiler_params=pltpu.CompilerParams(vmem_limit_bytes=40 << 20),
        name="attend",
    )(queries, kv)


def query_rows(query, positions):
    rows = query.shape[0]
    cosine, sine = tables(positions, ROPE_DIM)
    heads = query.reshape(rows, 4, NOPE + ROPE_DIM)
    turned = rotate(heads[..., NOPE:].astype(jnp.float32), cosine[:, None, :], sine[:, None, :])
    turned = turned.astype(jnp.bfloat16).transpose(1, 0, 2)
    flat = heads[..., :NOPE].transpose(1, 0, 2)
    out = []
    for p in range(2):
        for j in range(4):
            for i in range(2):
                h = 2 * p + i
                nope = jnp.pad(flat[h], ((0, 0), (64 * i, 64 - 64 * i)))
                rope = jnp.pad(turned[h], ((0, 0), (32 * j, 96 - 32 * j)))
                out.append(jnp.concatenate([nope, rope], axis=1))
    return jnp.stack(out).reshape(2, 4, 256, 256)


def mixer_half(query, latent, rope_key, latent_gain, key_up, value_up, out_proj):
    rows = query.shape[0]
    own_rows = latent.shape[0]
    query_start = lax.axis_index("ep") * rows
    key_start = query_start + lax.axis_index("tp") * own_rows
    normed = rms_scale(latent, latent_gain).astype(jnp.bfloat16)
    key_cos, key_sin = tables(key_start + jnp.arange(own_rows, dtype=jnp.int32), ROPE_DIM)
    rotated_key = rotate(rope_key.astype(jnp.float32), key_cos, key_sin).astype(jnp.bfloat16)
    queries = query_rows(query, query_start + jnp.arange(rows, dtype=jnp.int32))
    group_latent, group_rope = in_one_piece((normed, rotated_key), "tp", 0, 1)
    keys = jnp.dot(group_latent, key_up, preferred_element_type=jnp.float32).astype(jnp.bfloat16)
    values = lax.dot_general(
        value_up, group_latent, (((0,), (1,)), ((), ())), preferred_element_type=jnp.float32
    ).astype(jnp.bfloat16)
    rope = group_rope.reshape(4, 32, 32).transpose(1, 0, 2).reshape(32, 128)
    kv = jnp.concatenate([keys[:, :128], keys[:, 128:], values, rope], axis=0)
    kv = lax.all_gather(kv, "ep", axis=0)
    attention = attend(queries, kv)
    own_attention = lax.all_to_all(attention, "tp", split_axis=0, concat_axis=1, tiled=True)
    return jnp.dot(own_attention, out_proj, preferred_element_type=jnp.float32).astype(jnp.bfloat16)


def exchange(nx, where, share, w_gate, w_up, w_down):
    width = nx.shape[1] // 4
    units = w_gate.shape[1]
    ranks = lax.axis_size("ep")
    depth = ranks // 8
    f32, bf16 = jnp.float32, jnp.bfloat16

    def kernel(
        nx_ref, where_ref, share_ref, wg_hbm, wu_hbm, wd_hbm, o_ref,
        xn, pos, shr, slab, rows, wg, wu, wd, hid, back, ret, moved, final, mix,
        load_sem, own_sem, small_recv, arrive, ret_sem, ring_recv, send_sem,
    ):
        me, t = lax.axis_index("ep"), lax.axis_index("tp")
        z = me // 8
        right, left = lax.rem(t + 1, 4), lax.rem(t + 3, 4)

        loads = [
            pltpu.make_async_copy(wg_hbm, wg, load_sem.at[0]),
            pltpu.make_async_copy(wu_hbm, wu, load_sem.at[1]),
            pltpu.make_async_copy(wd_hbm.at[:, pl.ds(pl.multiple_of(t * width, width), width)], wd.at[t], load_sem.at[2]),
        ]
        for c in loads:
            c.start()

        barrier = pltpu.get_barrier_semaphore()

        def greet(k, _):
            pl.semaphore_signal(barrier, inc=1, device_id=(lax.rem(me + k, ranks), t), device_id_type=MESH)
            return 0

        lax.fori_loop(1, ranks, greet, 0)
        for k in range(1, 4):
            pl.semaphore_signal(barrier, inc=1, device_id=(me, lax.rem(t + k, 4)), device_id_type=MESH)
        pl.semaphore_wait(barrier, ranks + 2)

        def remote(s, d, send, recv, e, x):
            return pltpu.make_async_remote_copy(
                src_ref=s, dst_ref=d, send_sem=send, recv_sem=recv, device_id=(e, x), device_id_type=MESH
            )

        def cols(x):
            return pl.ds(pl.multiple_of(x * width, width), width)

        def small(k, kind):
            x = lax.rem(t + k, 4)
            send, recv = send_sem.at[6 + 3 * kind + k - 1], small_recv.at[kind, t]
            if kind == 0:
                return remote(nx_ref.at[:, cols(x)], xn.at[t], send, recv, me, x)
            if kind == 1:
                return remote(where_ref, pos.at[t], send, recv, me, x)
            if kind == 2:
                return remote(share_ref, shr.at[t], send, recv, me, x)
            if kind == 3:
                return remote(wd_hbm.at[:, cols(x)], wd.at[t], send, recv, me, x)
            return remote(moved.at[x], final.at[:, cols(t)], send, recv, me, x)

        def small_arrived(k, kind):
            x = lax.rem(t + k, 4)
            recv = small_recv.at[kind, x]
            ref = (xn.at[x], pos.at[x], shr.at[x], wd.at[x], final.at[:, cols(x)])[kind]
            return remote(ref, ref, send_sem.at[5], recv, me, x)

        for kind in range(4):
            for k in (1, 3, 2):
                small(k, kind).start()
        xn[t] = nx_ref[:, cols(t)]
        pos[t] = where_ref[...]
        shr[t] = share_ref[...]
        for kind in range(3):
            for k in range(1, 4):
                small_arrived(k, kind).wait_recv()

        place = pos[0] + pos[1] + pos[2] + pos[3] - 1
        first, second = place[0:1], place[1:2]
        tokens = xn[...].reshape(256, width)

        def offset(i):
            half = (i + 1) // 2
            return jnp.where(lax.rem(i, 2) == 1, depth // 2 - half, depth // 2 + half)

        def own_slab():
            return pltpu.make_async_copy(slab.at[me], rows.at[t, me], own_sem.at[0])

        def dispatch(i, _):
            zd = lax.rem(z + offset(i), depth)
            row = lax.broadcasted_iota(jnp.int32, (128, 256), 0) + zd * 128
            table = jnp.where((row == first) | (row == second), 1.0, 0.0).astype(bf16)
            out = jnp.dot(table, tokens, preferred_element_type=f32).astype(bf16)
            slab[pl.ds(zd * 8, 8)] = out.reshape(8, 16, width)

            def send(k, _):
                dst = zd * 8 + k

                @pl.when(dst != me)
                def _():
                    remote(slab.at[dst], rows.at[t, me], send_sem.at[0], arrive.at[me], dst, t).start()

                return 0

            lax.fori_loop(0, 8, send, 0)
            return 0

        lax.fori_loop(0, depth, dispatch, 0)
        own_slab().start()

        def ring(kind, chunk, block, d):
            buf = rows if kind < 2 else hid
            to = right if d == 0 else left
            origin = t if kind % 2 == 0 else (left if d == 0 else right)
            part = pl.ds(block * 8, 8) if kind % 2 == 0 else pl.ds(block * 8 + 4 * d, 4)
            ref = buf.at[origin, part]
            return remote(ref, ref, send_sem.at[1 + kind], ring_recv.at[kind, d, chunk], me, to)

        def ring_arrived(kind, chunk, block, d):
            buf = rows if kind < 2 else hid
            origin = (left if d == 0 else right) if kind % 2 == 0 else lax.rem(t + 2, 4)
            part = pl.ds(block * 8, 8) if kind % 2 == 0 else pl.ds(block * 8 + 4 * d, 4)
            ref = buf.at[origin, part]
            return remote(ref, ref, send_sem.at[5], ring_recv.at[kind, d, chunk], me, left)

        for c in loads:
            c.wait()

        def block_of(chunk):
            return lax.rem(z - offset(chunk) + depth, depth)

        def stage(s, _):
            @pl.when(s < depth)
            def _():
                block = block_of(s)

                def got(k, _):
                    e = block * 8 + k

                    @pl.when(e != me)
                    def _():
                        remote(rows.at[t, e], rows.at[t, e], send_sem.at[5], arrive.at[e], e, t).wait_recv()

                    @pl.when(e == me)
                    def _():
                        own_slab().wait()

                    return 0

                lax.fori_loop(0, 8, got, 0)
                for d in range(2):
                    ring(0, s, block, d).start()

            @pl.when((s >= 1) & (s < depth + 1))
            def _():
                block = block_of(s - 1)
                for d in range(2):
                    ring_arrived(0, s - 1, block, d).wait_recv()
                    ring(1, s - 1, block, d).start()

            @pl.when((s >= 2) & (s < depth + 2))
            def _():
                block = block_of(s - 2)
                for d in range(2):
                    ring_arrived(1, s - 2, block, d).wait_recv()
                gate = jnp.zeros((128, units), f32)
                up = jnp.zeros((128, units), f32)
                for x in range(4):
                    part = rows[x, pl.ds(block * 8, 8)].reshape(128, width)
                    gate = gate + jnp.dot(part, wg[width * x : width * x + width], preferred_element_type=f32)
                    up = up + jnp.dot(part, wu[width * x : width * x + width], preferred_element_type=f32)
                hidden = (gate / (1.0 + jnp.exp(-gate)) * up).astype(bf16)
                hid[t, pl.ds(block * 8, 8)] = hidden.reshape(8, 16, units)
                for d in range(2):
                    ring(2, s - 2, block, d).start()

            @pl.when((s >= 3) & (s < depth + 3))
            def _():
                block = block_of(s - 3)
                for d in range(2):
                    ring_arrived(2, s - 3, block, d).wait_recv()
                    ring(3, s - 3, block, d).start()

            @pl.when(s == 4)
            def _():
                for k in range(1, 4):
                    small_arrived(k, 3).wait_recv()

            @pl.when(s >= 4)
            def _():
                block = block_of(s - 4)
                for d in range(2):
                    ring_arrived(3, s - 4, block, d).wait_recv()
                total = jnp.zeros((128, width), f32)
                for x in range(4):
                    part = hid[x, pl.ds(block * 8, 8)].reshape(128, units)
                    total = total + jnp.dot(part, wd[x], preferred_element_type=f32).astype(bf16).astype(f32)
                back[pl.ds(block * 8, 8)] = total.astype(bf16).reshape(8, 16, width)

                def send(k, _):
                    e = block * 8 + k

                    @pl.when(e != me)
                    def _():
                        remote(back.at[e], ret.at[me], send_sem.at[21], ret_sem.at[me], e, t).start()

                    return 0

                lax.fori_loop(0, 8, send, 0)

            return 0

        lax.fori_loop(0, depth + 4, stage, 0)

        portion = shr[0] + shr[1] + shr[2] + shr[3]
        high = portion.astype(bf16).astype(f32)
        low = portion - high
        for c in range(4):
            row = lax.broadcasted_iota(jnp.int32, (ranks * 4, 256), 0) + c * ranks * 4
            for n, part in enumerate((high, low)):
                table = jnp.where(row == first, part[0:1], 0.0) + jnp.where(row == second, part[1:2], 0.0)
                mix[n, :, c * ranks * 4 : (c + 1) * ranks * 4] = table.T.astype(bf16)
        ret[me] = back[me]

        def came(e, _):
            @pl.when(e != me)
            def _():
                remote(ret.at[e], ret.at[e], send_sem.at[5], ret_sem.at[e], e, t).wait_recv()

            return 0

        lax.fori_loop(0, ranks, came, 0)
        given = ret[...].reshape(ranks * 16, width)
        summed = jnp.dot(mix[0], given, preferred_element_type=f32) + jnp.dot(
            mix[1], given, preferred_element_type=f32
        )
        moved[...] = summed.astype(bf16).reshape(4, 64, width)
        for k in (1, 3, 2):
            small(k, 4).start()
        final[:, cols(t)] = moved[t]
        for k in range(1, 4):
            small_arrived(k, 4).wait_recv()
        o_ref[...] = final[...]

        def drain(ref, sem):
            remote(ref, ref, sem, arrive.at[0], me, left).wait_send()

        drain(slab.at[pl.ds(0, ranks - 1)], send_sem.at[0])
        drain(rows.at[pl.ds(0, 2)], send_sem.at[1])
        drain(rows.at[0], send_sem.at[2])
        drain(hid.at[pl.ds(0, 2)], send_sem.at[3])
        drain(hid.at[0], send_sem.at[4])
        drain(back.at[pl.ds(0, ranks - 1)], send_sem.at[21])
        for kind in range(5):
            for k in range(1, 4):
                small(k, kind).wait_send()

    vmem = pl.BlockSpec(memory_space=pltpu.VMEM)
    hbm = pl.BlockSpec(memory_space=pl.ANY)
    return pl.pallas_call(
        kernel,
        out_shape=jax.ShapeDtypeStruct(nx.shape, bf16),
        in_specs=[vmem, vmem, vmem, hbm, hbm, hbm],
        out_specs=vmem,
        scratch_shapes=[
            pltpu.VMEM((4, 64, width), bf16),
            pltpu.VMEM((4, 8, 256), jnp.int32),
            pltpu.VMEM((4, 8, 256), f32),
            pltpu.VMEM((ranks, 16, width), bf16),
            pltpu.VMEM((4, ranks, 16, width), bf16),
            pltpu.VMEM(w_gate.shape, bf16),
            pltpu.VMEM(w_up.shape, bf16),
            pltpu.VMEM((4, units, width), bf16),
            pltpu.VMEM((4, ranks, 16, units), bf16),
            pltpu.VMEM((ranks, 16, width), bf16),
            pltpu.VMEM((ranks, 16, width), bf16),
            pltpu.VMEM((4, 64, width), bf16),
            pltpu.VMEM(nx.shape, bf16),
            pltpu.VMEM((2, 256, ranks * 16), bf16),
            pltpu.SemaphoreType.DMA((3,)),
            pltpu.SemaphoreType.DMA((1,)),
            pltpu.SemaphoreType.DMA((5, 4)),
            pltpu.SemaphoreType.DMA((ranks,)),
            pltpu.SemaphoreType.DMA((ranks,)),
            pltpu.SemaphoreType.DMA((4, 2, 8)),
            pltpu.SemaphoreType.DMA((22,)),
        ],
        compiler_params=pltpu.CompilerParams(
            collective_id=0, has_side_effects=True, vmem_limit_bytes=40 << 20
        ),
        cost_estimate=pl.CostEstimate(flops=5 * 10**9, bytes_accessed=3 * 10**7, transcendentals=0),
        name="exchange",
    )(nx, where, share, w_gate, w_up, w_down)


def expert_half(tokens, moe_gain, routes, group_prob, expert_prob, w_gate, w_up, w_down):
    row_count = tokens.shape[0]
    expert_count = lax.axis_size("ep")
    nx = rms_scale(tokens, moe_gain).astype(jnp.bfloat16)
    flat = routes.reshape(-1)
    onehot = (flat[:, None] == jnp.arange(expert_count, dtype=jnp.int32)[None, :]).astype(jnp.int32)
    earlier = jnp.cumsum(onehot, axis=0) - onehot
    slot = jnp.sum(earlier * onehot, axis=1)
    t = lax.axis_index("tp")
    target = (flat * 16 + t * 4 + slot + 1).reshape(row_count, 2).T
    shares = (group_prob[:, None] * expert_prob / jnp.sum(expert_prob, axis=1, keepdims=True)).T
    mine = (jnp.arange(256, dtype=jnp.int32) // 64 == t)[None, :]
    where = jnp.pad(jnp.where(mine, jnp.tile(target, (1, 4)), 0), ((0, 6), (0, 0)))
    share = jnp.pad(jnp.where(mine, jnp.tile(shares, (1, 4)), 0.0), ((0, 6), (0, 0)))
    return exchange(nx, where, share, w_gate[0], w_up[0], w_down[0])


def body(
    query,
    latent,
    rope_key,
    latent_gain,
    key_up,
    value_up,
    out_proj,
    tokens,
    moe_gain,
    routes,
    group_prob,
    expert_prob,
    w_gate,
    w_up,
    w_down,
):
    mixed = mixer_half(query, latent, rope_key, latent_gain, key_up, value_up, out_proj)
    moe_out = expert_half(tokens, moe_gain, routes, group_prob, expert_prob, w_gate, w_up, w_down)
    return (mixed, moe_out)


def solution(mesh):
    return jax.shard_map(
        body,
        mesh=mesh,
        in_specs=(
            P("ep", "tp"),
            P(("ep", "tp"), None),
            P(("ep", "tp"), None),
            P(),
            P(None, "tp"),
            P(None, "tp"),
            P(),
            P(("ep", "tp"), None),
            P(),
            P(("ep", "tp"), None),
            P(("ep", "tp")),
            P(("ep", "tp"), None),
            P("ep", None, "tp"),
            P("ep", None, "tp"),
            P("ep", "tp", None),
        ),
        out_specs=(P(("ep", "tp"), None), P(("ep", "tp"), None)),
        check_vma=False,
    )
```

```python
import math

import jax
import jax.numpy as jnp
from jax import lax
from jax.experimental import pallas as pl
from jax.experimental.pallas import tpu as pltpu
from jax.sharding import PartitionSpec as P

NOPE = 64
ROPE_DIM = 32
MESH = pl.DeviceIdType.MESH


epsilon = 1e-06
rope_base = 10000.0
masked_value = -1e30


def rms_scale(values, gain):
    widened = values.astype(jnp.float32)
    return widened * lax.rsqrt(jnp.mean(widened * widened, axis=-1, keepdims=True) + epsilon) * gain


def tables(positions, rope_width):
    half_width = rope_width // 2
    inverse = rope_base ** (-2.0 * jnp.arange(half_width, dtype=jnp.float32) / rope_width)
    angles = positions.astype(jnp.float32)[:, None] * inverse[None, :]
    return (jnp.cos(angles), jnp.sin(angles))


def rotate(values, cosine, sine):
    half_width = values.shape[-1] // 2
    lower = values[..., :half_width]
    upper = values[..., half_width:]
    return jnp.concatenate([lower * cosine - upper * sine, lower * sine + upper * cosine], axis=-1)


def query_rows(query, positions):
    rows = query.shape[0]
    cosine, sine = tables(positions, ROPE_DIM)
    heads = query.reshape(rows, 4, NOPE + ROPE_DIM)
    turned = rotate(heads[..., NOPE:].astype(jnp.float32), cosine[:, None, :], sine[:, None, :])
    turned = turned.astype(jnp.bfloat16).transpose(1, 0, 2)
    flat = heads[..., :NOPE].transpose(1, 0, 2)
    out = []
    for p in range(2):
        for j in range(4):
            for i in range(2):
                h = 2 * p + i
                nope = jnp.pad(flat[h], ((0, 0), (64 * i, 64 - 64 * i)))
                rope = jnp.pad(turned[h], ((0, 0), (32 * j, 96 - 32 * j)))
                out.append(jnp.concatenate([nope, rope], axis=1))
    return jnp.stack(out).reshape(2, 4, 256, 256)


def mixer_inputs(query, latent, rope_key, latent_gain):
    rows = query.shape[0]
    own_rows = latent.shape[0]
    t = lax.axis_index("tp")
    query_start = lax.axis_index("ep") * rows
    key_start = query_start + t * own_rows
    normed = rms_scale(latent, latent_gain).astype(jnp.bfloat16)
    key_cos, key_sin = tables(key_start + jnp.arange(own_rows, dtype=jnp.int32), ROPE_DIM)
    rotated = rotate(rope_key.astype(jnp.float32), key_cos, key_sin)
    mine = (jnp.arange(128, dtype=jnp.int32) // 32 == t)[None, :]
    packed = jnp.where(mine, jnp.tile(rotated, (1, 4)), 0.0).astype(jnp.bfloat16)
    queries = query_rows(query, query_start + jnp.arange(rows, dtype=jnp.int32))
    return queries, jnp.concatenate([normed, packed], axis=1)


def exchange(nx, where, share, latents, queries, w_gate, w_up, w_down, key_up, value_up, out_proj):
    width = nx.shape[1] // 4
    units = w_gate.shape[1]
    ranks = lax.axis_size("ep")
    depth = ranks // 8
    f32, bf16 = jnp.float32, jnp.bfloat16
    shift = math.log2(math.e) / math.sqrt(NOPE + ROPE_DIM)

    def kernel(
        nx_ref, where_ref, share_ref, lat_ref, q_ref, wg_hbm, wu_hbm, wd_hbm, ku_hbm, vu_hbm, wp_hbm, mixed_ref, o_ref,
        xn, pos, shr, slab, rows, wg, wu, wd, hid, back, ret, moved, final, mix,
        lat, ku, vu, wp, kv, top, total, acc, attm, attx,
        load_sem, own_sem, small_recv, arrive, ret_sem, ring_recv, send_sem, kv_recv, kv_send,
    ):
        me, t = lax.axis_index("ep"), lax.axis_index("tp")
        z = me // 8
        y, c = lax.rem(me, 8) // 2, lax.rem(me, 2)
        g0 = lax.rem(me, 8)
        right, left = lax.rem(t + 1, 4), lax.rem(t + 3, 4)

        loads = [
            pltpu.make_async_copy(wg_hbm, wg, load_sem.at[0]),
            pltpu.make_async_copy(wu_hbm, wu, load_sem.at[1]),
            pltpu.make_async_copy(wd_hbm.at[:, pl.ds(pl.multiple_of(t * width, width), width)], wd.at[t], load_sem.at[2]),
            pltpu.make_async_copy(wp_hbm, wp, load_sem.at[3]),
        ]
        early = [
            pltpu.make_async_copy(ku_hbm, ku, load_sem.at[4]),
            pltpu.make_async_copy(vu_hbm, vu, load_sem.at[5]),
        ]
        for load in early + loads:
            load.start()

        barrier = pltpu.get_barrier_semaphore()

        def greet(k, _):
            pl.semaphore_signal(barrier, inc=1, device_id=(lax.rem(me + k, ranks), t), device_id_type=MESH)
            return 0

        lax.fori_loop(1, ranks, greet, 0)
        for k in range(1, 4):
            pl.semaphore_signal(barrier, inc=1, device_id=(me, lax.rem(t + k, 4)), device_id_type=MESH)
        pl.semaphore_wait(barrier, ranks + 2)

        def remote(s, d, send, recv, e, x):
            return pltpu.make_async_remote_copy(
                src_ref=s, dst_ref=d, send_sem=send, recv_sem=recv, device_id=(e, x), device_id_type=MESH
            )

        def cols(x):
            return pl.ds(pl.multiple_of(x * width, width), width)

        def small(k, kind):
            x = lax.rem(t + k, 4)
            send, recv = send_sem.at[6 + 3 * kind + k - 1], small_recv.at[kind, t]
            if kind == 0:
                return remote(nx_ref.at[:, cols(x)], xn.at[t], send, recv, me, x)
            if kind == 1:
                return remote(where_ref, pos.at[t], send, recv, me, x)
            if kind == 2:
                return remote(share_ref, shr.at[t], send, recv, me, x)
            if kind == 3:
                return remote(wd_hbm.at[:, cols(x)], wd.at[t], send, recv, me, x)
            if kind == 4:
                return remote(moved.at[x], final.at[:, cols(t)], send, recv, me, x)
            if kind == 5:
                return remote(lat_ref, lat.at[t], send, recv, me, x)
            return remote(attm.at[x], attx.at[t], send, recv, me, x)

        def small_arrived(k, kind):
            x = lax.rem(t + k, 4)
            recv = small_recv.at[kind, x]
            ref = (xn.at[x], pos.at[x], shr.at[x], wd.at[x], final.at[:, cols(x)], lat.at[x], attx.at[x])[kind]
            return remote(ref, ref, send_sem.at[5], recv, me, x)

        for kind in (0, 1, 5, 2, 3):
            for k in (1, 3, 2):
                small(k, kind).start()
        lat[t] = lat_ref[...]
        xn[t] = nx_ref[:, cols(t)]
        pos[t] = where_ref[...]
        shr[t] = share_ref[...]
        for kind in range(2):
            for k in range(1, 4):
                small_arrived(k, kind).wait_recv()

        place = pos[0] + pos[1] + pos[2] + pos[3] - 1
        first, second = place[0:1], place[1:2]
        tokens = xn[...].reshape(256, width)

        def offset(i):
            half = (i + 1) // 2
            return jnp.where(lax.rem(i, 2) == 1, depth // 2 - half, depth // 2 + half)

        def own_slab():
            return pltpu.make_async_copy(slab.at[me], rows.at[t, me], own_sem.at[0])

        def dispatch(i, _):
            zd = lax.rem(z + offset(i), depth)
            row = lax.broadcasted_iota(jnp.int32, (128, 256), 0) + zd * 128
            table = jnp.where((row == first) | (row == second), 1.0, 0.0).astype(bf16)
            out = jnp.dot(table, tokens, preferred_element_type=f32).astype(bf16)
            slab[pl.ds(zd * 8, 8)] = out.reshape(8, 16, width)

            def send(k, _):
                dst = zd * 8 + k

                @pl.when(dst != me)
                def _():
                    remote(slab.at[dst], rows.at[t, me], send_sem.at[0], arrive.at[me], dst, t).start()

                return 0

            lax.fori_loop(0, 8, send, 0)
            return 0

        def plane(dz):
            return lax.rem(z + dz + depth, depth)

        def column(dy, flip=0):
            return lax.rem(y + dy + 4, 4) * 2 + (c if flip == 0 else 1 - c)

        def along_z(d, step, arrived=False):
            sign = 1 if d == 0 else -1
            block = plane(-sign * (step if arrived else step - 1))
            ref = kv.at[g0, block] if step < 4 else kv.at[g0, block, pl.ds(272 * d, 272)]
            n = 4 * d + step - 1
            return remote(ref, ref, kv_send.at[n], kv_recv.at[n], plane(sign) * 8 + g0, t)

        def along_y(d, stage, arrived=False):
            sign = 1 if d == 0 else -1
            hops = stage + (1 if arrived else 0)
            col = column(-sign * hops)
            ref = kv.at[col] if stage == 0 else kv.at[col, pl.ds(4 * d, 4)]
            n = 8 + 2 * stage + d
            return remote(ref, ref, kv_send.at[n], kv_recv.at[n], z * 8 + column(sign), t)

        def across(i, arrived=False):
            ref = kv.at[column((0, -1, 1, 2)[i], 1 if arrived else 0)]
            return remote(ref, ref, kv_send.at[12 + i], kv_recv.at[12 + i], z * 8 + column(0, 1), t)

        dispatch(0, 0)
        for k in range(1, 4):
            small_arrived(k, 5).wait_recv()
        for load in early:
            load.wait()
        flat = lat[...].reshape(128, lat.shape[2])
        latent = flat[:, : ku.shape[0]]
        keys = jnp.dot(latent, ku[...], preferred_element_type=f32).astype(bf16)
        values = jnp.dot(latent, vu[...], preferred_element_type=f32)
        kv[g0, z, 0:128] = keys[:, :128]
        kv[g0, z, 128:256] = keys[:, 128:]
        kv[g0, z, 256:512] = values.T.astype(bf16)
        packed = lat[0, :, ku.shape[0] :].astype(f32)
        for x in range(1, 4):
            packed = packed + lat[x, :, ku.shape[0] :].astype(f32)
        kv[g0, z, 512:544] = packed.astype(bf16)
        for d in range(2):
            along_z(d, 1).start()
        for step in range(1, 4):
            lax.fori_loop(2 * step - 1, 2 * step + 1, dispatch, 0)
            for d in range(2):
                along_z(d, step, True).wait_recv()
                along_z(d, step + 1).start()
        dispatch(depth - 1, 0)
        own_slab().start()
        for k in range(1, 4):
            small_arrived(k, 2).wait_recv()
        top[...] = jnp.full(top.shape, masked_value, f32)
        total[...] = jnp.zeros(total.shape, f32)
        acc[...] = jnp.zeros(acc.shape, f32)

        def attend(k, _):
            for i, at in enumerate((1, 4, 5, 7)):

                @pl.when(k == at)
                def _():
                    across(i, True).wait_recv()

            dy = jnp.where(k < 2, 0, jnp.where(k >= 6, 2, jnp.where(lax.rem(k, 2) == 0, 3, 1)))
            flip = (k == 1) | (k == 4) | (k == 5) | (k == 7)
            col = lax.rem(y + dy, 4) * 2 + jnp.where(flip, 1 - c, c)
            rope = kv[col, :, 512:544, :].reshape(256, 128)
            for p in range(2):
                parts = []
                for j in range(4):
                    some = kv[col, :, 128 * p + 32 * j : 128 * p + 32 * j + 32, :]
                    both = jnp.concatenate([some.reshape(256, 128), rope], axis=1)
                    s = lax.dot_general(both, q_ref[p, j], (((1,), (1,)), ((), ())), preferred_element_type=f32)
                    s = s.reshape(8, 32, 256)
                    place = lax.broadcasted_iota(jnp.int32, s.shape, 0) * 1024 + lax.broadcasted_iota(jnp.int32, s.shape, 1)
                    query = lax.broadcasted_iota(jnp.int32, s.shape, 2) & 127
                    parts.append(jnp.where(place - query <= (me - col) * 128 - 32 * j, s, masked_value))
                peak = parts[0].max(axis=0)
                for s in parts[1:]:
                    peak = jnp.maximum(peak, s.max(axis=0))
                before = top[p]
                peak = jnp.maximum(before, peak.max(axis=0, keepdims=True))
                factor = jnp.exp2((before - peak) * shift)
                added = jnp.zeros((32, 256), f32)
                raised = []
                for s in parts:
                    r = jnp.exp2((s - peak[None]) * shift)
                    added = added + r.sum(axis=0)
                    raised.append(r.astype(bf16))
                total[p] = total[p] * factor + added.sum(axis=0, keepdims=True)
                top[p] = peak
                weights = jnp.concatenate(raised, axis=1)
                update = acc[p] * factor
                for r in range(0, 8, 2):
                    vals = jnp.concatenate(
                        [kv[col, r + i, 256 + 128 * p : 384 + 128 * p, :] for i in range(2)], axis=1
                    )
                    update = update + jnp.dot(vals, weights[r : r + 2].reshape(256, 256), preferred_element_type=f32)
                acc[p] = update
            return 0

        def attended():
            pieces = []
            for p in range(2):
                a, l = acc[p], total[p]
                for i in range(2):
                    lanes = slice(128 * i, 128 * i + 128)
                    pieces.append(a[64 * i : 64 * i + 64, lanes] / l[:, lanes])
            attm[...] = jnp.concatenate(pieces, axis=0).T.astype(bf16).reshape(4, 32, 256)
            for k in (1, 3, 2):
                small(k, 6).start()
            attx[t] = attm[t]

        def ring(kind, chunk, block, d):
            buf = rows if kind < 2 else hid
            to = right if d == 0 else left
            origin = t if kind % 2 == 0 else (left if d == 0 else right)
            part = pl.ds(block * 8, 8) if kind % 2 == 0 else pl.ds(block * 8 + 4 * d, 4)
            ref = buf.at[origin, part]
            return remote(ref, ref, send_sem.at[1 + kind], ring_recv.at[kind, d, chunk], me, to)

        def ring_arrived(kind, chunk, block, d):
            buf = rows if kind < 2 else hid
            origin = (left if d == 0 else right) if kind % 2 == 0 else lax.rem(t + 2, 4)
            part = pl.ds(block * 8, 8) if kind % 2 == 0 else pl.ds(block * 8 + 4 * d, 4)
            ref = buf.at[origin, part]
            return remote(ref, ref, send_sem.at[5], ring_recv.at[kind, d, chunk], me, left)

        for load in loads:
            load.wait()

        def block_of(chunk):
            return lax.rem(z - offset(chunk) + depth, depth)

        def pick(s, table):
            out = jnp.int32(0)
            for at, value in table:
                out = jnp.where(s == at, value, out)
            return out

        def stage(s, _):
            @pl.when(s == 1)
            def _():
                for d in range(2):
                    along_z(d, 4, True).wait_recv()
                for d in range(2):
                    along_y(d, 0).start()
                across(0).start()

            @pl.when(s < depth)
            def _():
                block = block_of(s)

                def got(k, _):
                    e = block * 8 + k

                    @pl.when(e != me)
                    def _():
                        remote(rows.at[t, e], rows.at[t, e], send_sem.at[5], arrive.at[e], e, t).wait_recv()

                    @pl.when(e == me)
                    def _():
                        own_slab().wait()

                    return 0

                lax.fori_loop(0, 8, got, 0)
                for d in range(2):
                    ring(0, s, block, d).start()

            @pl.when((s >= 1) & (s < depth + 1))
            def _():
                block = block_of(s - 1)
                for d in range(2):
                    ring_arrived(0, s - 1, block, d).wait_recv()
                    ring(1, s - 1, block, d).start()

            @pl.when((s >= 2) & (s < depth + 2))
            def _():
                block = block_of(s - 2)
                for d in range(2):
                    ring_arrived(1, s - 2, block, d).wait_recv()
                gate = jnp.zeros((128, units), f32)
                up = jnp.zeros((128, units), f32)
                for x in range(4):
                    part = rows[x, pl.ds(block * 8, 8)].reshape(128, width)
                    gate = gate + jnp.dot(part, wg[width * x : width * x + width], preferred_element_type=f32)
                    up = up + jnp.dot(part, wu[width * x : width * x + width], preferred_element_type=f32)
                hidden = (gate / (1.0 + jnp.exp(-gate)) * up).astype(bf16)
                hid[t, pl.ds(block * 8, 8)] = hidden.reshape(8, 16, units)
                for d in range(2):
                    ring(2, s - 2, block, d).start()

            @pl.when((s >= 3) & (s < depth + 3))
            def _():
                block = block_of(s - 3)
                for d in range(2):
                    ring_arrived(2, s - 3, block, d).wait_recv()
                    ring(3, s - 3, block, d).start()

            @pl.when(s == 4)
            def _():
                for k in range(1, 4):
                    small_arrived(k, 3).wait_recv()

            @pl.when(s >= 4)
            def _():
                block = block_of(s - 4)
                for d in range(2):
                    ring_arrived(3, s - 4, block, d).wait_recv()
                total = jnp.zeros((128, width), f32)
                for x in range(4):
                    part = hid[x, pl.ds(block * 8, 8)].reshape(128, units)
                    total = total + jnp.dot(part, wd[x], preferred_element_type=f32).astype(bf16).astype(f32)
                back[pl.ds(block * 8, 8)] = total.astype(bf16).reshape(8, 16, width)

                def send(k, _):
                    e = block * 8 + k

                    @pl.when(e != me)
                    def _():
                        remote(back.at[e], ret.at[me], send_sem.at[27], ret_sem.at[me], e, t).start()

                    return 0

                lax.fori_loop(0, 8, send, 0)

            @pl.when(s == 7)
            def _():
                for d in range(2):
                    along_y(d, 0, True).wait_recv()
                    along_y(d, 1).start()
                    across(1 + d).start()

            @pl.when(s == 10)
            def _():
                for d in range(2):
                    along_y(d, 1, True).wait_recv()
                across(3).start()

            lo = pick(s, ((3, 1), (8, 2), (9, 4), (10, 6), (11, 7)))
            hi = pick(s, ((2, 1), (3, 2), (8, 4), (9, 6), (10, 7), (11, 8)))
            lax.fori_loop(lo, hi, attend, 0)

            @pl.when(s == 11)
            def _():
                attended()

            return 0

        lax.fori_loop(0, depth + 4, stage, 0)

        portion = shr[0] + shr[1] + shr[2] + shr[3]
        high = portion.astype(bf16).astype(f32)
        low = portion - high
        for n4 in range(4):
            row = lax.broadcasted_iota(jnp.int32, (ranks * 4, 256), 0) + n4 * ranks * 4
            for n, part in enumerate((high, low)):
                table = jnp.where(row == first, part[0:1], 0.0) + jnp.where(row == second, part[1:2], 0.0)
                mix[n, :, n4 * ranks * 4 : (n4 + 1) * ranks * 4] = table.T.astype(bf16)
        ret[me] = back[me]

        def came(e, _):
            @pl.when(e != me)
            def _():
                remote(ret.at[e], ret.at[e], send_sem.at[5], ret_sem.at[e], e, t).wait_recv()

            return 0

        lax.fori_loop(0, ranks, came, 0)
        given = ret[...].reshape(ranks * 16, width)
        summed = jnp.dot(mix[0], given, preferred_element_type=f32) + jnp.dot(
            mix[1], given, preferred_element_type=f32
        )
        moved[...] = summed.astype(bf16).reshape(4, 64, width)
        for k in (1, 3, 2):
            small(k, 4).start()
        final[:, cols(t)] = moved[t]
        for k in range(1, 4):
            small_arrived(k, 6).wait_recv()
        for n in range(4):
            at = slice(n * width, n * width + width)
            out = jnp.zeros((32, width), f32)
            for x in range(4):
                out = out + jnp.dot(attx[x], wp[256 * x : 256 * x + 256, at], preferred_element_type=f32)
            mixed_ref[:, at] = out.astype(bf16)
        for k in range(1, 4):
            small_arrived(k, 4).wait_recv()
        o_ref[...] = final[...]

        def drain(ref, sem):
            remote(ref, ref, sem, arrive.at[0], me, left).wait_send()

        drain(slab.at[pl.ds(0, ranks - 1)], send_sem.at[0])
        drain(rows.at[pl.ds(0, 2)], send_sem.at[1])
        drain(rows.at[0], send_sem.at[2])
        drain(hid.at[pl.ds(0, 2)], send_sem.at[3])
        drain(hid.at[0], send_sem.at[4])
        drain(back.at[pl.ds(0, ranks - 1)], send_sem.at[27])
        for kind in range(7):
            for k in range(1, 4):
                small(k, kind).wait_send()
        for d in range(2):
            for step in range(1, 5):
                along_z(d, step).wait_send()
            for step in range(2):
                along_y(d, step).wait_send()
        for i in range(4):
            across(i).wait_send()

    vmem = pl.BlockSpec(memory_space=pltpu.VMEM)
    hbm = pl.BlockSpec(memory_space=pl.ANY)
    return pl.pallas_call(
        kernel,
        out_shape=(jax.ShapeDtypeStruct((32, nx.shape[1]), bf16), jax.ShapeDtypeStruct(nx.shape, bf16)),
        in_specs=[vmem] * 5 + [hbm] * 6,
        out_specs=(vmem, vmem),
        scratch_shapes=[
            pltpu.VMEM((4, 64, width), bf16),
            pltpu.VMEM((4, 8, 256), jnp.int32),
            pltpu.VMEM((4, 8, 256), f32),
            pltpu.VMEM((ranks, 16, width), bf16),
            pltpu.VMEM((4, ranks, 16, width), bf16),
            pltpu.VMEM(w_gate.shape, bf16),
            pltpu.VMEM(w_up.shape, bf16),
            pltpu.VMEM((4, units, width), bf16),
            pltpu.VMEM((4, ranks, 16, units), bf16),
            pltpu.VMEM((ranks, 16, width), bf16),
            pltpu.VMEM((ranks, 16, width), bf16),
            pltpu.VMEM((4, 64, width), bf16),
            pltpu.VMEM(nx.shape, bf16),
            pltpu.VMEM((2, 256, ranks * 16), bf16),
            pltpu.VMEM((4,) + latents.shape, bf16),
            pltpu.VMEM(key_up.shape, bf16),
            pltpu.VMEM(value_up.shape, bf16),
            pltpu.VMEM(out_proj.shape, bf16),
            pltpu.VMEM((8, depth, 544, 128), bf16),
            pltpu.VMEM((2, 1, 256), f32),
            pltpu.VMEM((2, 1, 256), f32),
            pltpu.VMEM((2, 128, 256), f32),
            pltpu.VMEM((4, 32, 256), bf16),
            pltpu.VMEM((4, 32, 256), bf16),
            pltpu.SemaphoreType.DMA((6,)),
            pltpu.SemaphoreType.DMA((1,)),
            pltpu.SemaphoreType.DMA((7, 4)),
            pltpu.SemaphoreType.DMA((ranks,)),
            pltpu.SemaphoreType.DMA((ranks,)),
            pltpu.SemaphoreType.DMA((4, 2, 8)),
            pltpu.SemaphoreType.DMA((28,)),
            pltpu.SemaphoreType.DMA((16,)),
            pltpu.SemaphoreType.DMA((16,)),
        ],
        compiler_params=pltpu.CompilerParams(
            collective_id=0, has_side_effects=True, vmem_limit_bytes=56 << 20
        ),
        cost_estimate=pl.CostEstimate(flops=5 * 10**9, bytes_accessed=3 * 10**7, transcendentals=0),
        name="exchange",
    )(nx, where, share, latents, queries, w_gate, w_up, w_down, key_up, value_up, out_proj)


def expert_inputs(tokens, moe_gain, routes, group_prob, expert_prob):
    row_count = tokens.shape[0]
    expert_count = lax.axis_size("ep")
    nx = rms_scale(tokens, moe_gain).astype(jnp.bfloat16)
    flat = routes.reshape(-1)
    onehot = (flat[:, None] == jnp.arange(expert_count, dtype=jnp.int32)[None, :]).astype(jnp.int32)
    earlier = jnp.cumsum(onehot, axis=0) - onehot
    slot = jnp.sum(earlier * onehot, axis=1)
    t = lax.axis_index("tp")
    target = (flat * 16 + t * 4 + slot + 1).reshape(row_count, 2).T
    shares = (group_prob[:, None] * expert_prob / jnp.sum(expert_prob, axis=1, keepdims=True)).T
    mine = (jnp.arange(256, dtype=jnp.int32) // 64 == t)[None, :]
    where = jnp.pad(jnp.where(mine, jnp.tile(target, (1, 4)), 0), ((0, 6), (0, 0)))
    share = jnp.pad(jnp.where(mine, jnp.tile(shares, (1, 4)), 0.0), ((0, 6), (0, 0)))
    return nx, where, share


def body(
    query,
    latent,
    rope_key,
    latent_gain,
    key_up,
    value_up,
    out_proj,
    tokens,
    moe_gain,
    routes,
    group_prob,
    expert_prob,
    w_gate,
    w_up,
    w_down,
):
    nx, where, share = expert_inputs(tokens, moe_gain, routes, group_prob, expert_prob)
    queries, latents = mixer_inputs(query, latent, rope_key, latent_gain)
    return exchange(
        nx, where, share, latents, queries, w_gate[0], w_up[0], w_down[0], key_up, value_up, out_proj
    )


def solution(mesh):
    return jax.shard_map(
        body,
        mesh=mesh,
        in_specs=(
            P("ep", "tp"),
            P(("ep", "tp"), None),
            P(("ep", "tp"), None),
            P(),
            P(None, "tp"),
            P(None, "tp"),
            P(),
            P(("ep", "tp"), None),
            P(),
            P(("ep", "tp"), None),
            P(("ep", "tp")),
            P(("ep", "tp"), None),
            P("ep", None, "tp"),
            P("ep", None, "tp"),
            P("ep", "tp", None),
        ),
        out_specs=(P(("ep", "tp"), None), P(("ep", "tp"), None)),
        check_vma=False,
    )
```

```python
import math

import jax
import jax.numpy as jnp
from jax import lax
from jax.experimental import pallas as pl
from jax.experimental.pallas import tpu as pltpu
from jax.sharding import PartitionSpec as P

NOPE = 64
ROPE_DIM = 32
MESH = pl.DeviceIdType.MESH

ZW = (0, 1, 2, 3)
SA = 5
SB = 9
SM = 1
SF = 10
LO = ((4, 1), (5, 2), (6, 3), (7, 4), (8, 5), (9, 6), (10, 7))
HI = ((3, 1), (4, 2), (5, 3), (6, 4), (7, 5), (8, 6), (9, 7), (10, 8))


epsilon = 1e-06
rope_base = 10000.0
masked_value = -1e30


def rotation(positions):
    half_width = ROPE_DIM // 2
    inverse = rope_base ** (-2.0 * jnp.arange(half_width, dtype=jnp.float32) / ROPE_DIM)
    angles = positions.astype(jnp.float32)[:, None] * inverse[None, :]
    cosine, sine = jnp.cos(angles), jnp.sin(angles)
    return jnp.concatenate([cosine, cosine, -sine, sine], axis=-1)


def plain_copy(first, second):
    def kernel(a_ref, b_ref, c_ref, d_ref):
        c_ref[...] = a_ref[...]
        d_ref[...] = b_ref[...]

    vmem = pl.BlockSpec(memory_space=pltpu.VMEM)
    return pl.pallas_call(
        kernel,
        out_shape=(
            jax.ShapeDtypeStruct(first.shape, first.dtype),
            jax.ShapeDtypeStruct(second.shape, second.dtype),
        ),
        in_specs=[vmem, vmem],
        out_specs=(vmem, vmem),
        name="plain_copy",
    )(first, second)


def exchange(
    tokens, moe_gain, routes, group_prob, expert_prob, turn, latent, rope_key, latent_gain,
    query, w_gate, w_up, w_down, key_up, value_up, out_proj,
):
    width = tokens.shape[1] // 4
    units = w_gate.shape[1]
    ranks = lax.axis_size("ep")
    depth = ranks // 8
    f32, bf16 = jnp.float32, jnp.bfloat16
    shift = math.log2(math.e) / math.sqrt(NOPE + ROPE_DIM)

    def kernel(
        tok_hbm, gain_ref, routes_ref, group_ref, prob_ref, turn_ref, lat_hbm, rope_hbm, lgain_ref,
        q_hbm, wg_hbm, wu_hbm, wd_hbm, ku_hbm, vu_hbm, wp_hbm, mixed_ref, o_ref,
        tok, lin, rin, qin, nx_ref, where_ref, share_ref, lat_ref, q_ref, relay,
        xn, pos, shr, slab, rows, wg, wu, wd, hid, back, ret, moved, final, mix,
        lat, ku, vu, wp, kv, top, total, acc, attm, attx,
        load_sem, own_sem, small_recv, arrive, ret_sem, ring_recv, send_sem, kv_recv, kv_send, relay_send, relay_recv,
    ):
        me, t = lax.axis_index("ep"), lax.axis_index("tp")
        z = me // 8
        y, c = lax.rem(me, 8) // 2, lax.rem(me, 2)
        g0 = lax.rem(me, 8)
        right, left = lax.rem(t + 1, 4), lax.rem(t + 3, 4)

        loads = [
            pltpu.make_async_copy(wg_hbm, wg, load_sem.at[0]),
            pltpu.make_async_copy(wu_hbm, wu, load_sem.at[1]),
            pltpu.make_async_copy(wd_hbm.at[:, pl.ds(pl.multiple_of(t * width, width), width)], wd.at[t], load_sem.at[2]),
            pltpu.make_async_copy(wp_hbm, wp, load_sem.at[3]),
        ]
        early = [
            pltpu.make_async_copy(ku_hbm, ku, load_sem.at[4]),
            pltpu.make_async_copy(vu_hbm, vu, load_sem.at[5]),
        ]
        first_loads = [
            pltpu.make_async_copy(tok_hbm, tok, load_sem.at[6]),
            pltpu.make_async_copy(lat_hbm, lin, load_sem.at[7]),
            pltpu.make_async_copy(rope_hbm, rin, load_sem.at[8]),
            pltpu.make_async_copy(q_hbm, qin, load_sem.at[9]),
        ]
        for load in first_loads + early + loads:
            load.start()

        barrier = pltpu.get_barrier_semaphore()

        def greet(k, _):
            pl.semaphore_signal(barrier, inc=1, device_id=(lax.rem(me + k, ranks), t), device_id_type=MESH)
            return 0

        lax.fori_loop(1, ranks, greet, 0)
        for k in range(1, 4):
            pl.semaphore_signal(barrier, inc=1, device_id=(me, lax.rem(t + k, 4)), device_id_type=MESH)

        def normed(ref, gain):
            wide = ref[...].astype(f32)
            return wide * lax.rsqrt(jnp.mean(wide * wide, axis=-1, keepdims=True) + epsilon) * gain[...]

        def turned(part, cosine, sine):
            half = ROPE_DIM // 2
            swapped = jnp.concatenate([part[:, half:], part[:, :half]], axis=1)
            return part * cosine + swapped * sine

        choice = routes_ref[...].astype(f32)
        down_at = lax.broadcasted_iota(jnp.int32, (64, 64), 0)
        across_at = lax.broadcasted_iota(jnp.int32, (64, 64), 1)
        columns = [
            jnp.sum(jnp.where(down_at == across_at, choice[k : k + 1], 0.0), axis=1, keepdims=True) for k in range(2)
        ]
        mine = lax.broadcasted_iota(jnp.int32, (1, 256), 1) // 64 == t
        odds = prob_ref[...]
        where_ref[...] = jnp.zeros(where_ref.shape, jnp.int32)
        share_ref[...] = jnp.zeros(share_ref.shape, f32)
        for k in range(2):
            row = choice[k : k + 1]
            same = jnp.where(columns[0] == row, 1.0, 0.0) + jnp.where(columns[1] == row, 1.0, 0.0)
            slot = jnp.sum(jnp.where(down_at < across_at, same, 0.0), axis=0, keepdims=True)
            target = (row * 16.0 + slot).astype(jnp.int32) + t * 4 + 1
            portion = group_ref[...] * odds[k : k + 1] / (odds[0:1] + odds[1:2])
            where_ref[k : k + 1] = jnp.where(mine, jnp.concatenate([target] * 4, axis=1), 0)
            share_ref[k : k + 1] = jnp.where(mine, jnp.concatenate([portion] * 4, axis=1), 0.0)
        for load in first_loads:
            load.wait()
        nx_ref[...] = normed(tok, gain_ref).astype(bf16)
        lat_ref[:, : lin.shape[1]] = normed(lin, lgain_ref).astype(bf16)
        table = turn_ref[pl.ds(pl.multiple_of(t * 32, 32), 32)]
        own_key = turned(rin[...].astype(f32), table[:, :32], table[:, 32:])
        own_lanes = lax.broadcasted_iota(jnp.int32, (32, 128), 1) // 32 == t
        lat_ref[:, lin.shape[1] :] = jnp.where(own_lanes, jnp.concatenate([own_key] * 4, axis=1), 0.0).astype(bf16)
        pl.semaphore_wait(barrier, ranks + 2)

        def remote(s, d, send, recv, e, x):
            return pltpu.make_async_remote_copy(
                src_ref=s, dst_ref=d, send_sem=send, recv_sem=recv, device_id=(e, x), device_id_type=MESH
            )

        def cols(x):
            return pl.ds(pl.multiple_of(x * width, width), width)

        def small(k, kind):
            x = lax.rem(t + k, 4)
            send, recv = send_sem.at[6 + 3 * kind + k - 1], small_recv.at[kind, t]
            if kind == 0:
                return remote(nx_ref.at[:, cols(x)], xn.at[t], send, recv, me, x)
            if kind == 1:
                return remote(where_ref, pos.at[t], send, recv, me, x)
            if kind == 2:
                return remote(share_ref, shr.at[t], send, recv, me, x)
            if kind == 3:
                return remote(wd_hbm.at[:, cols(x)], wd.at[t], send, recv, me, x)
            if kind == 4:
                return remote(moved.at[x], final.at[:, cols(t)], send, recv, me, x)
            if kind == 5:
                return remote(lat_ref, lat.at[t], send, recv, me, x)
            return remote(attm.at[x], attx.at[t], send, recv, me, x)

        def small_arrived(k, kind):
            x = lax.rem(t + k, 4)
            recv = small_recv.at[kind, x]
            ref = (xn.at[x], pos.at[x], shr.at[x], wd.at[x], final.at[:, cols(x)], lat.at[x], attx.at[x])[kind]
            return remote(ref, ref, send_sem.at[5], recv, me, x)

        def relayed(d, hop, arrived=False):
            to = right if d == 0 else left
            part = pl.ds(128 * d, 128)
            if hop == 0:
                source = relay.at[d] if arrived else wd_hbm.at[part, cols(lax.rem(t + 2, 4))]
                return remote(source, relay.at[d], relay_send.at[d], relay_recv.at[d], me, to)
            origin = lax.rem(t + 2, 4) if arrived else (left if d == 0 else right)
            target = wd.at[origin, part]
            return remote(target if arrived else relay.at[d], target, relay_send.at[2 + d], relay_recv.at[2 + d], me, to)

        for kind in (0, 1, 5, 2):
            for k in (1, 3, 2):
                small(k, kind).start()
        for d in range(2):
            relayed(d, 0).start()
        for k in (1, 3):
            small(k, 3).start()
        lat[t] = lat_ref[...]
        xn[t] = nx_ref[:, cols(t)]
        pos[t] = where_ref[...]
        shr[t] = share_ref[...]
        for kind in range(2):
            for k in range(1, 4):
                small_arrived(k, kind).wait_recv()

        place = pos[0] + pos[1] + pos[2] + pos[3] - 1
        first, second = place[0:1], place[1:2]
        tokens = xn[...].reshape(256, width)

        def offset(i):
            half = (i + 1) // 2
            return jnp.where(lax.rem(i, 2) == 1, depth // 2 - half, depth // 2 + half)

        def own_slab():
            return pltpu.make_async_copy(slab.at[me], rows.at[t, me], own_sem.at[0])

        def dispatch(i, _):
            zd = lax.rem(z + offset(i), depth)
            row = lax.broadcasted_iota(jnp.int32, (128, 256), 0) + zd * 128
            table = jnp.where((row == first) | (row == second), 1.0, 0.0).astype(bf16)
            out = jnp.dot(table, tokens, preferred_element_type=f32).astype(bf16)
            slab[pl.ds(zd * 8, 8)] = out.reshape(8, 16, width)

            def send(k, _):
                dst = zd * 8 + k

                @pl.when(dst != me)
                def _():
                    remote(slab.at[dst], rows.at[t, me], send_sem.at[0], arrive.at[me], dst, t).start()

                return 0

            lax.fori_loop(0, 8, send, 0)
            return 0

        def plane(dz):
            return lax.rem(z + dz + depth, depth)

        def column(dy, flip=0):
            return lax.rem(y + dy + 4, 4) * 2 + (c if flip == 0 else 1 - c)

        def along_z(d, step, arrived=False):
            sign = 1 if d == 0 else -1
            block = plane(-sign * (step if arrived else step - 1))
            ref = kv.at[g0, block] if step < 4 else kv.at[g0, block, pl.ds(272 * d, 272)]
            n = 4 * d + step - 1
            return remote(ref, ref, kv_send.at[n], kv_recv.at[n], plane(sign) * 8 + g0, t)

        def along_y(d, block, arrived=False):
            sign = 1 if d == 0 else -1
            ref = kv.at[column(-sign if arrived else 0), block]
            n = 8 + 8 * d + block
            return remote(ref, ref, kv_send.at[n], kv_recv.at[n], z * 8 + column(sign), t)

        def along_y2(d, arrived=False):
            sign = 1 if d == 0 else -1
            ref = kv.at[column(-sign * (2 if arrived else 1)), pl.ds(4 * d, 4)]
            return remote(ref, ref, kv_send.at[24 + d], kv_recv.at[24 + d], z * 8 + column(sign), t)

        def across(i, arrived=False):
            ref = kv.at[column((0, -1, 1, 2)[i], 1 if arrived else 0)]
            return remote(ref, ref, kv_send.at[26 + i], kv_recv.at[26 + i], z * 8 + column(0, 1), t)

        dispatch(0, 0)
        for k in range(1, 4):
            small_arrived(k, 5).wait_recv()
        for load in early:
            load.wait()
        flat = lat[...].reshape(128, lat.shape[2])
        latent = flat[:, : ku.shape[0]]
        keys = jnp.dot(latent, ku[...], preferred_element_type=f32).astype(bf16)
        values = jnp.dot(latent, vu[...], preferred_element_type=f32)
        kv[g0, z, 0:128] = keys[:, :128]
        kv[g0, z, 128:256] = keys[:, 128:]
        kv[g0, z, 256:512] = values.T.astype(bf16)
        packed = lat[0, :, ku.shape[0] :].astype(f32)
        for x in range(1, 4):
            packed = packed + lat[x, :, ku.shape[0] :].astype(f32)
        kv[g0, z, 512:544] = packed.astype(bf16)
        for d in range(2):
            along_z(d, 1).start()
            along_y(d, z).start()
        lax.fori_loop(1, depth, dispatch, 0)
        own_slab().start()
        for d in range(2):
            relayed(d, 0, True).wait_recv()
            relayed(d, 1).start()
        for k in range(1, 4):
            small_arrived(k, 2).wait_recv()
        q_ref[...] = jnp.zeros(q_ref.shape, bf16)
        asked = qin[...].astype(f32)
        for h in range(4):
            p, i = h // 2, h % 2
            nope = asked[:, 96 * h : 96 * h + 64].astype(bf16)
            rope = turned(asked[:, 96 * h + 64 : 96 * h + 96], turn_ref[:, :32], turn_ref[:, 32:]).astype(bf16)
            for j in range(4):
                q_ref[p, j, 128 * i : 128 * i + 128, 64 * i : 64 * i + 64] = nope
                q_ref[p, j, 128 * i : 128 * i + 128, 128 + 32 * j : 160 + 32 * j] = rope
        top[...] = jnp.full(top.shape, masked_value, f32)
        total[...] = jnp.zeros(total.shape, f32)
        acc[...] = jnp.zeros(acc.shape, f32)

        def attend(k, _):
            for i, at in enumerate((1, 4, 5, 7)):

                @pl.when(k == at)
                def _():
                    across(i, True).wait_recv()

            dy = jnp.where(k < 2, 0, jnp.where(k >= 6, 2, jnp.where(lax.rem(k, 2) == 0, 3, 1)))
            flip = (k == 1) | (k == 4) | (k == 5) | (k == 7)
            col = lax.rem(y + dy, 4) * 2 + jnp.where(flip, 1 - c, c)
            rope = kv[col, :, 512:544, :].reshape(256, 128)
            for p in range(2):
                parts = []
                for j in range(4):
                    some = kv[col, :, 128 * p + 32 * j : 128 * p + 32 * j + 32, :]
                    both = jnp.concatenate([some.reshape(256, 128), rope], axis=1)
                    s = lax.dot_general(both, q_ref[p, j], (((1,), (1,)), ((), ())), preferred_element_type=f32)
                    s = s.reshape(8, 32, 256)
                    place = lax.broadcasted_iota(jnp.int32, s.shape, 0) * 1024 + lax.broadcasted_iota(jnp.int32, s.shape, 1)
                    query = lax.broadcasted_iota(jnp.int32, s.shape, 2) & 127
                    parts.append(jnp.where(place - query <= (me - col) * 128 - 32 * j, s, masked_value))
                peak = parts[0].max(axis=0)
                for s in parts[1:]:
                    peak = jnp.maximum(peak, s.max(axis=0))
                before = top[p]
                peak = jnp.maximum(before, peak.max(axis=0, keepdims=True))
                factor = jnp.exp2((before - peak) * shift)
                added = jnp.zeros((32, 256), f32)
                raised = []
                for s in parts:
                    r = jnp.exp2((s - peak[None]) * shift)
                    added = added + r.sum(axis=0)
                    raised.append(r.astype(bf16))
                total[p] = total[p] * factor + added.sum(axis=0, keepdims=True)
                top[p] = peak
                weights = jnp.concatenate(raised, axis=1)
                update = acc[p] * factor
                for r in range(0, 8, 2):
                    vals = jnp.concatenate(
                        [kv[col, r + i, 256 + 128 * p : 384 + 128 * p, :] for i in range(2)], axis=1
                    )
                    update = update + jnp.dot(vals, weights[r : r + 2].reshape(256, 256), preferred_element_type=f32)
                acc[p] = update
            return 0

        def attended():
            pieces = []
            for p in range(2):
                a, l = acc[p], total[p]
                for i in range(2):
                    lanes = slice(128 * i, 128 * i + 128)
                    pieces.append(a[64 * i : 64 * i + 64, lanes] / l[:, lanes])
            attm[...] = jnp.concatenate(pieces, axis=0).T.astype(bf16).reshape(4, 32, 256)
            for k in (1, 3, 2):
                small(k, 6).start()
            attx[t] = attm[t]

        def ring(kind, chunk, block, d):
            buf = rows if kind < 2 else hid
            to = right if d == 0 else left
            origin = t if kind % 2 == 0 else (left if d == 0 else right)
            part = pl.ds(block * 8, 8) if kind % 2 == 0 else pl.ds(block * 8 + 4 * d, 4)
            ref = buf.at[origin, part]
            return remote(ref, ref, send_sem.at[1 + kind], ring_recv.at[kind, d, chunk], me, to)

        def ring_arrived(kind, chunk, block, d):
            buf = rows if kind < 2 else hid
            origin = (left if d == 0 else right) if kind % 2 == 0 else lax.rem(t + 2, 4)
            part = pl.ds(block * 8, 8) if kind % 2 == 0 else pl.ds(block * 8 + 4 * d, 4)
            ref = buf.at[origin, part]
            return remote(ref, ref, send_sem.at[5], ring_recv.at[kind, d, chunk], me, left)

        for load in loads:
            load.wait()

        def block_of(chunk):
            return lax.rem(z - offset(chunk) + depth, depth)

        def mix_tables():
            portion = shr[0] + shr[1] + shr[2] + shr[3]
            high = portion.astype(bf16).astype(f32)
            low = portion - high
            for n4 in range(4):
                row = lax.broadcasted_iota(jnp.int32, (ranks * 4, 256), 0) + n4 * ranks * 4
                for n, part in enumerate((high, low)):
                    table = jnp.where(row == first, part[0:1], 0.0) + jnp.where(row == second, part[1:2], 0.0)
                    mix[n, :, n4 * ranks * 4 : (n4 + 1) * ranks * 4] = table.T.astype(bf16)

        def pick(s, table):
            out = jnp.int32(0)
            for at, value in table:
                out = jnp.where(s == at, value, out)
            return out

        def stage(s, _):
            @pl.when(s < depth)
            def _():
                block = block_of(s)

                def got(k, _):
                    e = block * 8 + k

                    @pl.when(e != me)
                    def _():
                        remote(rows.at[t, e], rows.at[t, e], send_sem.at[5], arrive.at[e], e, t).wait_recv()

                    @pl.when(e == me)
                    def _():
                        own_slab().wait()

                    return 0

                lax.fori_loop(0, 8, got, 0)
                for d in range(2):
                    ring(0, s, block, d).start()

            @pl.when((s >= 1) & (s < depth + 1))
            def _():
                block = block_of(s - 1)
                for d in range(2):
                    ring_arrived(0, s - 1, block, d).wait_recv()
                    ring(1, s - 1, block, d).start()

            @pl.when((s >= 2) & (s < depth + 2))
            def _():
                block = block_of(s - 2)
                for d in range(2):
                    ring_arrived(1, s - 2, block, d).wait_recv()
                gate = jnp.zeros((128, units), f32)
                up = jnp.zeros((128, units), f32)
                for x in range(4):
                    part = rows[x, pl.ds(block * 8, 8)].reshape(128, width)
                    gate = gate + jnp.dot(part, wg[width * x : width * x + width], preferred_element_type=f32)
                    up = up + jnp.dot(part, wu[width * x : width * x + width], preferred_element_type=f32)
                hidden = (gate / (1.0 + jnp.exp(-gate)) * up).astype(bf16)
                hid[t, pl.ds(block * 8, 8)] = hidden.reshape(8, 16, units)
                for d in range(2):
                    ring(2, s - 2, block, d).start()

            @pl.when((s >= 3) & (s < depth + 3))
            def _():
                block = block_of(s - 3)
                for d in range(2):
                    ring_arrived(2, s - 3, block, d).wait_recv()
                    ring(3, s - 3, block, d).start()

            @pl.when(s == 4)
            def _():
                for k in (1, 3):
                    small_arrived(k, 3).wait_recv()
                for d in range(2):
                    relayed(d, 1, True).wait_recv()

            @pl.when(s >= 4)
            def _():
                block = block_of(s - 4)
                for d in range(2):
                    ring_arrived(3, s - 4, block, d).wait_recv()
                total = jnp.zeros((128, width), f32)
                for x in range(4):
                    part = hid[x, pl.ds(block * 8, 8)].reshape(128, units)
                    total = total + jnp.dot(part, wd[x], preferred_element_type=f32).astype(bf16).astype(f32)
                back[pl.ds(block * 8, 8)] = total.astype(bf16).reshape(8, 16, width)

                def send(k, _):
                    e = block * 8 + k

                    @pl.when(e != me)
                    def _():
                        remote(back.at[e], ret.at[me], send_sem.at[27], ret_sem.at[me], e, t).start()

                    return 0

                lax.fori_loop(0, 8, send, 0)

            for step in range(1, 5):

                @pl.when(s == ZW[step - 1])
                def _(step=step):
                    for d in range(2):
                        along_z(d, step, True).wait_recv()
                        if step < 4:
                            along_z(d, step + 1).start()
                    for block in (plane(-step), plane(step)) if step < 4 else (plane(4),):
                        for d in range(2):
                            along_y(d, block).start()
                    if step == 4:
                        across(0).start()

            @pl.when(s == SA)
            def _():
                for d in range(2):
                    lax.fori_loop(0, depth, lambda b, _, d=d: (along_y(d, b, True).wait_recv(), 0)[1], 0)
                    along_y2(d).start()
                    across(1 + d).start()

            @pl.when(s == SB)
            def _():
                for d in range(2):
                    along_y2(d, True).wait_recv()
                across(3).start()

            @pl.when(s == SM)
            def _():
                mix_tables()

            lax.fori_loop(pick(s, LO), pick(s, HI), attend, 0)

            @pl.when(s == SF)
            def _():
                attended()

            return 0

        lax.fori_loop(0, depth + 4, stage, 0)

        ret[me] = back[me]

        def came(e, _):
            @pl.when(e != me)
            def _():
                remote(ret.at[e], ret.at[e], send_sem.at[5], ret_sem.at[e], e, t).wait_recv()

            return 0

        lax.fori_loop(0, ranks, came, 0)
        given = ret[...].reshape(ranks * 16, width)
        summed = jnp.dot(mix[0], given, preferred_element_type=f32) + jnp.dot(
            mix[1], given, preferred_element_type=f32
        )
        moved[...] = summed.astype(bf16).reshape(4, 64, width)
        for k in (1, 3, 2):
            small(k, 4).start()
        final[:, cols(t)] = moved[t]
        for k in range(1, 4):
            small_arrived(k, 6).wait_recv()
        for n in range(4):
            at = slice(n * width, n * width + width)
            out = jnp.zeros((32, width), f32)
            for x in range(4):
                out = out + jnp.dot(attx[x], wp[256 * x : 256 * x + 256, at], preferred_element_type=f32)
            mixed_ref[:, at] = out.astype(bf16)
        for k in range(1, 4):
            small_arrived(k, 4).wait_recv()
        o_ref[...] = final[...]

        def drain(ref, sem):
            remote(ref, ref, sem, arrive.at[0], me, left).wait_send()

        drain(slab.at[pl.ds(0, ranks - 1)], send_sem.at[0])
        drain(rows.at[pl.ds(0, 2)], send_sem.at[1])
        drain(rows.at[0], send_sem.at[2])
        drain(hid.at[pl.ds(0, 2)], send_sem.at[3])
        drain(hid.at[0], send_sem.at[4])
        drain(back.at[pl.ds(0, ranks - 1)], send_sem.at[27])
        for kind in range(7):
            for k in range(1, 4):
                if (k, kind) != (2, 3):
                    small(k, kind).wait_send()
        for d in range(2):
            for hop in range(2):
                relayed(d, hop).wait_send()
        for d in range(2):
            for step in range(1, 5):
                along_z(d, step).wait_send()
            lax.fori_loop(0, depth, lambda b, _, d=d: (along_y(d, b).wait_send(), 0)[1], 0)
            along_y2(d).wait_send()
        for i in range(4):
            across(i).wait_send()

    vmem = pl.BlockSpec(memory_space=pltpu.VMEM)
    hbm = pl.BlockSpec(memory_space=pl.ANY)
    return pl.pallas_call(
        kernel,
        out_shape=(jax.ShapeDtypeStruct((32, tokens.shape[1]), bf16), jax.ShapeDtypeStruct(tokens.shape, bf16)),
        in_specs=[hbm] + [vmem] * 5 + [hbm] * 2 + [vmem] + [hbm] * 7,
        out_specs=(vmem, vmem),
        scratch_shapes=[
            pltpu.VMEM(tokens.shape, bf16),
            pltpu.VMEM(latent.shape, bf16),
            pltpu.VMEM(rope_key.shape, bf16),
            pltpu.VMEM(query.shape, bf16),
            pltpu.VMEM(tokens.shape, bf16),
            pltpu.VMEM((8, 256), jnp.int32),
            pltpu.VMEM((8, 256), f32),
            pltpu.VMEM((32, latent.shape[1] + 128), bf16),
            pltpu.VMEM((2, 4, 256, 256), bf16),
            pltpu.VMEM((2, 128, width), bf16),
            pltpu.VMEM((4, 64, width), bf16),
            pltpu.VMEM((4, 8, 256), jnp.int32),
            pltpu.VMEM((4, 8, 256), f32),
            pltpu.VMEM((ranks, 16, width), bf16),
            pltpu.VMEM((4, ranks, 16, width), bf16),
            pltpu.VMEM(w_gate.shape, bf16),
            pltpu.VMEM(w_up.shape, bf16),
            pltpu.VMEM((4, units, width), bf16),
            pltpu.VMEM((4, ranks, 16, units), bf16),
            pltpu.VMEM((ranks, 16, width), bf16),
            pltpu.VMEM((ranks, 16, width), bf16),
            pltpu.VMEM((4, 64, width), bf16),
            pltpu.VMEM(tokens.shape, bf16),
            pltpu.VMEM((2, 256, ranks * 16), bf16),
            pltpu.VMEM((4, 32, latent.shape[1] + 128), bf16),
            pltpu.VMEM(key_up.shape, bf16),
            pltpu.VMEM(value_up.shape, bf16),
            pltpu.VMEM(out_proj.shape, bf16),
            pltpu.VMEM((8, depth, 544, 128), bf16),
            pltpu.VMEM((2, 1, 256), f32),
            pltpu.VMEM((2, 1, 256), f32),
            pltpu.VMEM((2, 128, 256), f32),
            pltpu.VMEM((4, 32, 256), bf16),
            pltpu.VMEM((4, 32, 256), bf16),
            pltpu.SemaphoreType.DMA((10,)),
            pltpu.SemaphoreType.DMA((1,)),
            pltpu.SemaphoreType.DMA((7, 4)),
            pltpu.SemaphoreType.DMA((ranks,)),
            pltpu.SemaphoreType.DMA((ranks,)),
            pltpu.SemaphoreType.DMA((4, 2, 8)),
            pltpu.SemaphoreType.DMA((28,)),
            pltpu.SemaphoreType.DMA((30,)),
            pltpu.SemaphoreType.DMA((30,)),
            pltpu.SemaphoreType.DMA((4,)),
            pltpu.SemaphoreType.DMA((4,)),
        ],
        compiler_params=pltpu.CompilerParams(
            collective_id=0, has_side_effects=True, vmem_limit_bytes=56 << 20
        ),
        cost_estimate=pl.CostEstimate(flops=5 * 10**9, bytes_accessed=3 * 10**7, transcendentals=0),
        name="exchange",
    )(
        tokens, moe_gain, routes, group_prob, expert_prob, turn, latent, rope_key, latent_gain,
        query, w_gate, w_up, w_down, key_up, value_up, out_proj,
    )


def body(
    query,
    latent,
    rope_key,
    latent_gain,
    key_up,
    value_up,
    out_proj,
    tokens,
    moe_gain,
    routes,
    group_prob,
    expert_prob,
    w_gate,
    w_up,
    w_down,
):
    rows = query.shape[0]
    turn = rotation(lax.axis_index("ep") * rows + jnp.arange(rows, dtype=jnp.int32))
    mixed, moe_out = exchange(
        tokens, moe_gain[None], routes.T, group_prob[None], expert_prob.T, turn, latent, rope_key, latent_gain[None],
        query, w_gate[0], w_up[0], w_down[0], key_up, value_up, out_proj,
    )
    return plain_copy(mixed, moe_out)


def solution(mesh):
    return jax.shard_map(
        body,
        mesh=mesh,
        in_specs=(
            P("ep", "tp"),
            P(("ep", "tp"), None),
            P(("ep", "tp"), None),
            P(),
            P(None, "tp"),
            P(None, "tp"),
            P(),
            P(("ep", "tp"), None),
            P(),
            P(("ep", "tp"), None),
            P(("ep", "tp")),
            P(("ep", "tp"), None),
            P("ep", None, "tp"),
            P("ep", None, "tp"),
            P("ep", "tp", None),
        ),
        out_specs=(P(("ep", "tp"), None), P(("ep", "tp"), None)),
        check_vma=False,
    )
```

```python
import math

import jax
import jax.numpy as jnp
import numpy as np
from jax import lax
from jax.experimental import pallas as pl
from jax.experimental.pallas import tpu as pltpu
from jax.sharding import PartitionSpec as P

NOPE = 64
ROPE_DIM = 32
MESH = pl.DeviceIdType.MESH

ZW = (1, 2, 3, 4)
SA = 6
SB = 9
SM = 1
SF = 11
LO = ((5, 0), (7, 2), (8, 4), (10, 6), (11, 7))
HI = ((5, 2), (7, 4), (8, 6), (10, 7), (11, 8))


epsilon = 1e-06
rope_base = 10000.0
masked_value = -1e30


def rotation(positions):
    inverse = rope_base ** (-2.0 * np.arange(ROPE_DIM // 2) / ROPE_DIM)
    angles = np.tile(positions[:, None] * inverse[None, :], (1, 2))
    return jnp.asarray(np.concatenate([np.cos(angles), np.sin(angles)], axis=1), jnp.float32)


def plain_copy(first, second):
    def kernel(a_ref, b_ref, c_ref, d_ref):
        c_ref[...] = a_ref[...]
        d_ref[...] = b_ref[...]

    vmem = pl.BlockSpec(memory_space=pltpu.VMEM)
    return pl.pallas_call(
        kernel,
        out_shape=(
            jax.ShapeDtypeStruct(first.shape, first.dtype),
            jax.ShapeDtypeStruct(second.shape, second.dtype),
        ),
        in_specs=[vmem, vmem],
        out_specs=(vmem, vmem),
        name="plain_copy",
    )(first, second)


def exchange(
    tokens, moe_gain, routes, group_prob, expert_prob, within, starts, latent, rope_key, latent_gain,
    query, w_gate, w_up, w_down, key_up, value_up, out_proj,
):
    width = tokens.shape[1] // 4
    units = w_gate.shape[1]
    ranks = lax.axis_size("ep")
    depth = ranks // 8
    f32, bf16 = jnp.float32, jnp.bfloat16
    shift = math.log2(math.e) / math.sqrt(NOPE + ROPE_DIM)

    def kernel(
        tok_hbm, gain_ref, routes_ref, group_ref, prob_ref, within_ref, starts_ref, lat_hbm, rope_hbm, lgain_ref,
        q_hbm, wg_hbm, wu_hbm, wd_hbm, ku_hbm, vu_hbm, wp_hbm, mixed_ref, o_ref,
        tok, lin, rin, qin, nx_ref, note_ref, lat_ref, q_ref, turn_ref,
        xn, note, slab, rows, wg, wu, wd, hid, back, ret, moved, final, mix,
        lat, ku, vu, wp, kv, top, total, acc, attm, attx,
        load_sem, own_sem, small_recv, arrive, ret_sem, ring_recv, send_sem, kv_recv, kv_send,
    ):
        me, t = lax.axis_index("ep"), lax.axis_index("tp")
        z = me // 8
        y, c = lax.rem(me, 8) // 2, lax.rem(me, 2)
        g0 = lax.rem(me, 8)
        right, left = lax.rem(t + 1, 4), lax.rem(t + 3, 4)

        loads = [
            pltpu.make_async_copy(wg_hbm, wg, load_sem.at[0]),
            pltpu.make_async_copy(wu_hbm, wu, load_sem.at[1]),
            pltpu.make_async_copy(wd_hbm.at[:, pl.ds(pl.multiple_of(t * width, width), width)], wd.at[t], load_sem.at[2]),
            pltpu.make_async_copy(wp_hbm, wp, load_sem.at[3]),
        ]
        early = [
            pltpu.make_async_copy(ku_hbm, ku, load_sem.at[4]),
            pltpu.make_async_copy(vu_hbm, vu, load_sem.at[5]),
        ]
        first_loads = [
            pltpu.make_async_copy(tok_hbm, tok, load_sem.at[6]),
            pltpu.make_async_copy(lat_hbm, lin, load_sem.at[7]),
            pltpu.make_async_copy(rope_hbm, rin, load_sem.at[8]),
            pltpu.make_async_copy(q_hbm, qin, load_sem.at[9]),
        ]
        for load in first_loads + early + loads:
            load.start()

        barrier = pltpu.get_barrier_semaphore()

        def greet(k, _):
            pl.semaphore_signal(barrier, inc=1, device_id=(lax.rem(me + k, ranks), t), device_id_type=MESH)
            return 0

        lax.fori_loop(1, ranks, greet, 0)
        for k in range(1, 4):
            pl.semaphore_signal(barrier, inc=1, device_id=(me, lax.rem(t + k, 4)), device_id_type=MESH)

        def normed(ref, gain):
            wide = ref[...].astype(f32)
            return wide * lax.rsqrt(jnp.mean(wide * wide, axis=-1, keepdims=True) + epsilon) * gain[...]

        def turned(part, cosine, sine):
            half = ROPE_DIM // 2
            swapped = jnp.concatenate([part[:, half:], part[:, :half]], axis=1)
            return part * cosine + swapped * sine

        choice = routes_ref[...].astype(f32)
        down_at = lax.broadcasted_iota(jnp.int32, (64, 64), 0)
        across_at = lax.broadcasted_iota(jnp.int32, (64, 64), 1)
        columns = [
            jnp.sum(jnp.where(down_at == across_at, choice[k : k + 1], 0.0), axis=1, keepdims=True) for k in range(2)
        ]
        odds = prob_ref[...]
        note_ref[...] = jnp.zeros(note_ref.shape, f32)
        for k in range(2):
            row = choice[k : k + 1]
            same = jnp.where(columns[0] == row, 1.0, 0.0) + jnp.where(columns[1] == row, 1.0, 0.0)
            slot = jnp.sum(jnp.where(down_at < across_at, same, 0.0), axis=0, keepdims=True)
            note_ref[k : k + 1, 0:64] = row * 16.0 + slot + (t * 4).astype(f32)
            note_ref[2 + k : 3 + k, 0:64] = group_ref[...] * odds[k : k + 1] / (odds[0:1] + odds[1:2])
        for load in first_loads:
            load.wait()
        nx_ref[...] = normed(tok, gain_ref).astype(bf16)
        lat_ref[:, : lin.shape[1]] = normed(lin, lgain_ref).astype(bf16)
        near, far = within_ref[...], starts_ref[pl.ds(me, 1)]
        near_cos, near_sin, far_cos, far_sin = near[:, :32], near[:, 32:], far[:, :32], far[:, 32:]
        sine = near_sin * far_cos + near_cos * far_sin
        lower = lax.broadcasted_iota(jnp.int32, sine.shape, 1) < ROPE_DIM // 2
        turn_ref[:, :32] = near_cos * far_cos - near_sin * far_sin
        turn_ref[:, 32:] = jnp.where(lower, -sine, sine)
        table = turn_ref[pl.ds(pl.multiple_of(t * 32, 32), 32)]
        own_key = turned(rin[...].astype(f32), table[:, :32], table[:, 32:])
        own_lanes = lax.broadcasted_iota(jnp.int32, (32, 128), 1) // 32 == t
        lat_ref[:, lin.shape[1] :] = jnp.where(own_lanes, jnp.concatenate([own_key] * 4, axis=1), 0.0).astype(bf16)
        pl.semaphore_wait(barrier, ranks + 2)

        def remote(s, d, send, recv, e, x):
            return pltpu.make_async_remote_copy(
                src_ref=s, dst_ref=d, send_sem=send, recv_sem=recv, device_id=(e, x), device_id_type=MESH
            )

        def cols(x):
            return pl.ds(pl.multiple_of(x * width, width), width)

        def small(k, kind):
            x = lax.rem(t + k, 4)
            send, recv = send_sem.at[6 + 3 * kind + k - 1], small_recv.at[kind, t]
            if kind == 0:
                return remote(nx_ref.at[:, cols(x)], xn.at[t], send, recv, me, x)
            if kind == 1:
                return remote(note_ref, note.at[t], send, recv, me, x)
            if kind == 3:
                return remote(wd_hbm.at[:, cols(x)], wd.at[t], send, recv, me, x)
            if kind == 4:
                return remote(moved.at[x], final.at[:, cols(t)], send, recv, me, x)
            if kind == 5:
                return remote(lat_ref, lat.at[t], send, recv, me, x)
            return remote(attm.at[x], attx.at[t], send, recv, me, x)

        def small_arrived(k, kind):
            x = lax.rem(t + k, 4)
            recv = small_recv.at[kind, x]
            ref = (xn.at[x], note.at[x], None, wd.at[x], final.at[:, cols(x)], lat.at[x], attx.at[x])[kind]
            return remote(ref, ref, send_sem.at[5], recv, me, x)

        for kind in (0, 1, 5, 3):
            for k in (2, 1, 3):
                small(k, kind).start()
        lat[t] = lat_ref[...]
        xn[t] = nx_ref[:, cols(t)]
        note[t] = note_ref[...]
        for kind in range(2):
            for k in range(1, 4):
                small_arrived(k, kind).wait_recv()

        notes = jnp.concatenate([note[x, :, 0:64] for x in range(4)], axis=1)
        first, second = notes[0:1].astype(jnp.int32), notes[1:2].astype(jnp.int32)
        tokens = xn[...].reshape(256, width)

        def offset(i):
            return jnp.where(i == 6, 7, jnp.where(i == 5, 1, jnp.where(i == 4, 5, jnp.where(i == 3, 3, jnp.where(i == 2, 4, jnp.where(i == 1, 6, jnp.where(i == 0, 2, jnp.int32(0))))))))

        def own_slab():
            return pltpu.make_async_copy(slab.at[me], rows.at[t, me], own_sem.at[0])

        def dispatch(i, _):
            zd = lax.rem(z + offset(i), depth)
            row = lax.broadcasted_iota(jnp.int32, (128, 256), 0) + zd * 128
            table = jnp.where((row == first) | (row == second), 1.0, 0.0).astype(bf16)
            out = jnp.dot(table, tokens, preferred_element_type=f32).astype(bf16)
            slab[pl.ds(zd * 8, 8)] = out.reshape(8, 16, width)

            def send(k, _):
                dst = zd * 8 + k

                @pl.when(dst != me)
                def _():
                    remote(slab.at[dst], rows.at[t, me], send_sem.at[0], arrive.at[me], dst, t).start()

                return 0

            lax.fori_loop(0, 8, send, 0)
            return 0

        def plane(dz):
            return lax.rem(z + dz + depth, depth)

        def column(dy, flip=0):
            return lax.rem(y + dy + 4, 4) * 2 + (c if flip == 0 else 1 - c)

        def along_z(d, step, arrived=False):
            sign = 1 if d == 0 else -1
            block = plane(-sign * (step if arrived else step - 1))
            ref = kv.at[g0, block] if step < 4 else kv.at[g0, block, pl.ds(272 * d, 272)]
            n = 4 * d + step - 1
            return remote(ref, ref, kv_send.at[n], kv_recv.at[n], plane(sign) * 8 + g0, t)

        def along_y(d, block, arrived=False):
            sign = 1 if d == 0 else -1
            ref = kv.at[column(-sign if arrived else 0), block]
            n = 8 + 8 * d + block
            return remote(ref, ref, kv_send.at[n], kv_recv.at[n], z * 8 + column(sign), t)

        def along_y2(d, arrived=False):
            sign = 1 if d == 0 else -1
            ref = kv.at[column(-sign * (2 if arrived else 1)), pl.ds(4 * d, 4)]
            return remote(ref, ref, kv_send.at[24 + d], kv_recv.at[24 + d], z * 8 + column(sign), t)

        def across(i, arrived=False):
            ref = kv.at[column((0, -1, 1, 2)[i], 1 if arrived else 0)]
            return remote(ref, ref, kv_send.at[26 + i], kv_recv.at[26 + i], z * 8 + column(0, 1), t)

        dispatch(0, 0)
        for k in range(1, 4):
            small_arrived(k, 5).wait_recv()
        for load in early:
            load.wait()
        flat = lat[...].reshape(128, lat.shape[2])
        latent = flat[:, : ku.shape[0]]
        keys = jnp.dot(latent, ku[...], preferred_element_type=f32).astype(bf16)
        values = jnp.dot(latent, vu[...], preferred_element_type=f32)
        kv[g0, z, 0:128] = keys[:, :128]
        kv[g0, z, 128:256] = keys[:, 128:]
        kv[g0, z, 256:512] = values.T.astype(bf16)
        packed = lat[0, :, ku.shape[0] :].astype(f32)
        for x in range(1, 4):
            packed = packed + lat[x, :, ku.shape[0] :].astype(f32)
        kv[g0, z, 512:544] = packed.astype(bf16)
        for d in range(2):
            along_z(d, 1).start()
            along_y(d, z).start()
        lax.fori_loop(1, depth, dispatch, 0)
        own_slab().start()
        q_ref[...] = jnp.zeros(q_ref.shape, bf16)
        asked = qin[...].astype(f32)
        for h in range(4):
            p, i = h // 2, h % 2
            nope = asked[:, 96 * h : 96 * h + 64].astype(bf16)
            rope = turned(asked[:, 96 * h + 64 : 96 * h + 96], turn_ref[:, :32], turn_ref[:, 32:]).astype(bf16)
            for j in range(4):
                q_ref[p, j, 128 * i : 128 * i + 128, 64 * i : 64 * i + 64] = nope
                q_ref[p, j, 128 * i : 128 * i + 128, 128 + 32 * j : 160 + 32 * j] = rope
        top[...] = jnp.full(top.shape, masked_value, f32)
        total[...] = jnp.zeros(total.shape, f32)
        acc[...] = jnp.zeros(acc.shape, f32)

        def attend(k, _):
            for i, at in enumerate((1, 4, 5, 7)):

                @pl.when(k == at)
                def _():
                    across(i, True).wait_recv()

            dy = jnp.where(k < 2, 0, jnp.where(k >= 6, 2, jnp.where(lax.rem(k, 2) == 0, 3, 1)))
            flip = (k == 1) | (k == 4) | (k == 5) | (k == 7)
            col = lax.rem(y + dy, 4) * 2 + jnp.where(flip, 1 - c, c)
            rope = kv[col, :, 512:544, :].reshape(256, 128)
            for p in range(2):
                parts = []
                for j in range(4):
                    some = kv[col, :, 128 * p + 32 * j : 128 * p + 32 * j + 32, :]
                    both = jnp.concatenate([some.reshape(256, 128), rope], axis=1)
                    s = lax.dot_general(both, q_ref[p, j], (((1,), (1,)), ((), ())), preferred_element_type=f32)
                    s = s.reshape(8, 32, 256)
                    place = lax.broadcasted_iota(jnp.int32, s.shape, 0) * 1024 + lax.broadcasted_iota(jnp.int32, s.shape, 1)
                    query = lax.broadcasted_iota(jnp.int32, s.shape, 2) & 127
                    parts.append(jnp.where(place - query <= (me - col) * 128 - 32 * j, s, masked_value))
                peak = parts[0].max(axis=0)
                for s in parts[1:]:
                    peak = jnp.maximum(peak, s.max(axis=0))
                before = top[p]
                peak = jnp.maximum(before, peak.max(axis=0, keepdims=True))
                factor = jnp.exp2((before - peak) * shift)
                added = jnp.zeros((32, 256), f32)
                raised = []
                for s in parts:
                    r = jnp.exp2((s - peak[None]) * shift)
                    added = added + r.sum(axis=0)
                    raised.append(r.astype(bf16))
                total[p] = total[p] * factor + added.sum(axis=0, keepdims=True)
                top[p] = peak
                weights = jnp.concatenate(raised, axis=1)
                update = acc[p] * factor
                for r in range(0, 8, 2):
                    vals = jnp.concatenate(
                        [kv[col, r + i, 256 + 128 * p : 384 + 128 * p, :] for i in range(2)], axis=1
                    )
                    update = update + jnp.dot(vals, weights[r : r + 2].reshape(256, 256), preferred_element_type=f32)
                acc[p] = update
            return 0

        def attended():
            pieces = []
            for p in range(2):
                a, l = acc[p], total[p]
                for i in range(2):
                    lanes = slice(128 * i, 128 * i + 128)
                    pieces.append(a[64 * i : 64 * i + 64, lanes] / l[:, lanes])
            attm[...] = jnp.concatenate(pieces, axis=0).T.astype(bf16).reshape(4, 32, 256)
            for k in (1, 3, 2):
                small(k, 6).start()
            attx[t] = attm[t]

        def ring(kind, chunk, block, d):
            buf = rows if kind < 2 else hid
            to = right if d == 0 else left
            origin = t if kind % 2 == 0 else (left if d == 0 else right)
            part = pl.ds(block * 8, 8) if kind % 2 == 0 else pl.ds(block * 8 + 4 * d, 4)
            ref = buf.at[origin, part]
            return remote(ref, ref, send_sem.at[1 + kind], ring_recv.at[kind, d, chunk], me, to)

        def ring_arrived(kind, chunk, block, d):
            buf = rows if kind < 2 else hid
            origin = (left if d == 0 else right) if kind % 2 == 0 else lax.rem(t + 2, 4)
            part = pl.ds(block * 8, 8) if kind % 2 == 0 else pl.ds(block * 8 + 4 * d, 4)
            ref = buf.at[origin, part]
            return remote(ref, ref, send_sem.at[5], ring_recv.at[kind, d, chunk], me, left)

        for load in loads:
            load.wait()

        def block_of(chunk):
            return lax.rem(z - offset(chunk) + depth, depth)

        def mix_tables():
            for n4 in range(4):
                row = lax.broadcasted_iota(jnp.int32, (ranks * 4, 256), 0) + n4 * ranks * 4
                table = jnp.where(row == first, notes[2:3], 0.0) + jnp.where(row == second, notes[3:4], 0.0)
                mix[:, n4 * ranks * 4 : (n4 + 1) * ranks * 4] = table.T.astype(bf16)

        def pick(s, table):
            out = jnp.int32(0)
            for at, value in table:
                out = jnp.where(s == at, value, out)
            return out

        def stage(s, _):
            @pl.when(s < depth)
            def _():
                block = block_of(s)

                def got(k, _):
                    e = block * 8 + k

                    @pl.when(e != me)
                    def _():
                        remote(rows.at[t, e], rows.at[t, e], send_sem.at[5], arrive.at[e], e, t).wait_recv()

                    @pl.when(e == me)
                    def _():
                        own_slab().wait()

                    return 0

                lax.fori_loop(0, 8, got, 0)
                for d in range(2):
                    ring(0, s, block, d).start()

            @pl.when((s >= 1) & (s < depth + 1))
            def _():
                block = block_of(s - 1)
                for d in range(2):
                    ring_arrived(0, s - 1, block, d).wait_recv()
                    ring(1, s - 1, block, d).start()

            @pl.when((s >= 2) & (s < depth + 2))
            def _():
                block = block_of(s - 2)
                for d in range(2):
                    ring_arrived(1, s - 2, block, d).wait_recv()
                gate = jnp.zeros((128, units), f32)
                up = jnp.zeros((128, units), f32)
                for x in range(4):
                    part = rows[x, pl.ds(block * 8, 8)].reshape(128, width)
                    gate = gate + jnp.dot(part, wg[width * x : width * x + width], preferred_element_type=f32)
                    up = up + jnp.dot(part, wu[width * x : width * x + width], preferred_element_type=f32)
                hidden = (gate / (1.0 + jnp.exp(-gate)) * up).astype(bf16)
                hid[t, pl.ds(block * 8, 8)] = hidden.reshape(8, 16, units)
                for d in range(2):
                    ring(2, s - 2, block, d).start()

            @pl.when((s >= 3) & (s < depth + 3))
            def _():
                block = block_of(s - 3)
                for d in range(2):
                    ring_arrived(2, s - 3, block, d).wait_recv()
                    ring(3, s - 3, block, d).start()

            @pl.when(s == 4)
            def _():
                for k in range(1, 4):
                    small_arrived(k, 3).wait_recv()

            @pl.when(s >= 4)
            def _():
                block = block_of(s - 4)
                for d in range(2):
                    ring_arrived(3, s - 4, block, d).wait_recv()
                total = jnp.zeros((128, width), f32)
                for x in range(4):
                    part = hid[x, pl.ds(block * 8, 8)].reshape(128, units)
                    total = total + jnp.dot(part, wd[x], preferred_element_type=f32).astype(bf16).astype(f32)
                back[pl.ds(block * 8, 8)] = total.astype(bf16).reshape(8, 16, width)

                def send(k, _):
                    e = block * 8 + k

                    @pl.when(e != me)
                    def _():
                        remote(back.at[e], ret.at[me], send_sem.at[27], ret_sem.at[me], e, t).start()

                    return 0

                lax.fori_loop(0, 8, send, 0)

            for step in range(1, 5):

                @pl.when(s == ZW[step - 1])
                def _(step=step):
                    for d in range(2):
                        along_z(d, step, True).wait_recv()
                        if step < 4:
                            along_z(d, step + 1).start()
                    for block in (plane(-step), plane(step)) if step < 4 else (plane(4),):
                        for d in range(2):
                            along_y(d, block).start()
                    if step == 4:
                        across(0).start()

            @pl.when(s == SA)
            def _():
                for d in range(2):
                    lax.fori_loop(0, depth, lambda b, _, d=d: (along_y(d, b, True).wait_recv(), 0)[1], 0)
                    along_y2(d).start()
                    across(1 + d).start()

            @pl.when(s == SB)
            def _():
                for d in range(2):
                    along_y2(d, True).wait_recv()
                across(3).start()

            @pl.when(s == SM)
            def _():
                mix_tables()

            lax.fori_loop(pick(s, LO), pick(s, HI), attend, 0)

            @pl.when(s == SF)
            def _():
                attended()

            return 0

        lax.fori_loop(0, depth + 4, stage, 0)

        ret[me] = back[me]

        def came(e, _):
            @pl.when(e != me)
            def _():
                remote(ret.at[e], ret.at[e], send_sem.at[5], ret_sem.at[e], e, t).wait_recv()

            return 0

        lax.fori_loop(0, ranks, came, 0)
        given = ret[...].reshape(ranks * 16, width)
        summed = jnp.dot(mix[...], given, preferred_element_type=f32)
        moved[...] = summed.astype(bf16).reshape(4, 64, width)
        for k in (1, 3, 2):
            small(k, 4).start()
        final[:, cols(t)] = moved[t]
        for k in range(1, 4):
            small_arrived(k, 6).wait_recv()
        for n in range(4):
            at = slice(n * width, n * width + width)
            out = jnp.zeros((32, width), f32)
            for x in range(4):
                out = out + jnp.dot(attx[x], wp[256 * x : 256 * x + 256, at], preferred_element_type=f32)
            mixed_ref[:, at] = out.astype(bf16)
        for k in range(1, 4):
            small_arrived(k, 4).wait_recv()
        o_ref[...] = final[...]

        def drain(ref, sem):
            remote(ref, ref, sem, arrive.at[0], me, left).wait_send()

        drain(slab.at[pl.ds(0, ranks - 1)], send_sem.at[0])
        drain(rows.at[pl.ds(0, 2)], send_sem.at[1])
        drain(rows.at[0], send_sem.at[2])
        drain(hid.at[pl.ds(0, 2)], send_sem.at[3])
        drain(hid.at[0], send_sem.at[4])
        drain(back.at[pl.ds(0, ranks - 1)], send_sem.at[27])
        for kind in (0, 1, 3, 4, 5, 6):
            for k in range(1, 4):
                small(k, kind).wait_send()
        for d in range(2):
            for step in range(1, 5):
                along_z(d, step).wait_send()
            lax.fori_loop(0, depth, lambda b, _, d=d: (along_y(d, b).wait_send(), 0)[1], 0)
            along_y2(d).wait_send()
        for i in range(4):
            across(i).wait_send()

    vmem = pl.BlockSpec(memory_space=pltpu.VMEM)
    hbm = pl.BlockSpec(memory_space=pl.ANY)
    return pl.pallas_call(
        kernel,
        out_shape=(jax.ShapeDtypeStruct((32, tokens.shape[1]), bf16), jax.ShapeDtypeStruct(tokens.shape, bf16)),
        in_specs=[hbm] + [vmem] * 6 + [hbm] * 2 + [vmem] + [hbm] * 7,
        out_specs=(vmem, vmem),
        scratch_shapes=[
            pltpu.VMEM(tokens.shape, bf16),
            pltpu.VMEM(latent.shape, bf16),
            pltpu.VMEM(rope_key.shape, bf16),
            pltpu.VMEM(query.shape, bf16),
            pltpu.VMEM(tokens.shape, bf16),
            pltpu.VMEM((8, 128), f32),
            pltpu.VMEM((32, latent.shape[1] + 128), bf16),
            pltpu.VMEM((2, 4, 256, 256), bf16),
            pltpu.VMEM((128, 64), f32),
            pltpu.VMEM((4, 64, width), bf16),
            pltpu.VMEM((4, 8, 128), f32),
            pltpu.VMEM((ranks, 16, width), bf16),
            pltpu.VMEM((4, ranks, 16, width), bf16),
            pltpu.VMEM(w_gate.shape, bf16),
            pltpu.VMEM(w_up.shape, bf16),
            pltpu.VMEM((4, units, width), bf16),
            pltpu.VMEM((4, ranks, 16, units), bf16),
            pltpu.VMEM((ranks, 16, width), bf16),
            pltpu.VMEM((ranks, 16, width), bf16),
            pltpu.VMEM((4, 64, width), bf16),
            pltpu.VMEM(tokens.shape, bf16),
            pltpu.VMEM((256, ranks * 16), bf16),
            pltpu.VMEM((4, 32, latent.shape[1] + 128), bf16),
            pltpu.VMEM(key_up.shape, bf16),
            pltpu.VMEM(value_up.shape, bf16),
            pltpu.VMEM(out_proj.shape, bf16),
            pltpu.VMEM((8, depth, 544, 128), bf16),
            pltpu.VMEM((2, 1, 256), f32),
            pltpu.VMEM((2, 1, 256), f32),
            pltpu.VMEM((2, 128, 256), f32),
            pltpu.VMEM((4, 32, 256), bf16),
            pltpu.VMEM((4, 32, 256), bf16),
            pltpu.SemaphoreType.DMA((10,)),
            pltpu.SemaphoreType.DMA((1,)),
            pltpu.SemaphoreType.DMA((7, 4)),
            pltpu.SemaphoreType.DMA((ranks,)),
            pltpu.SemaphoreType.DMA((ranks,)),
            pltpu.SemaphoreType.DMA((4, 2, 8)),
            pltpu.SemaphoreType.DMA((28,)),
            pltpu.SemaphoreType.DMA((30,)),
            pltpu.SemaphoreType.DMA((30,)),
        ],
        compiler_params=pltpu.CompilerParams(
            collective_id=0, has_side_effects=True, vmem_limit_bytes=56 << 20
        ),
        cost_estimate=pl.CostEstimate(flops=5 * 10**9, bytes_accessed=3 * 10**7, transcendentals=0),
        name="exchange",
    )(
        tokens, moe_gain, routes, group_prob, expert_prob, within, starts, latent, rope_key, latent_gain,
        query, w_gate, w_up, w_down, key_up, value_up, out_proj,
    )


def body(
    query,
    latent,
    rope_key,
    latent_gain,
    key_up,
    value_up,
    out_proj,
    tokens,
    moe_gain,
    routes,
    group_prob,
    expert_prob,
    w_gate,
    w_up,
    w_down,
):
    rows = query.shape[0]
    within, starts = rotation(np.arange(rows)), rotation(np.arange(lax.axis_size("ep")) * rows)
    mixed, moe_out = exchange(
        tokens, moe_gain[None], routes.T, group_prob[None], expert_prob.T, within, starts, latent, rope_key, latent_gain[None],
        query, w_gate[0], w_up[0], w_down[0], key_up, value_up, out_proj,
    )
    return plain_copy(mixed, moe_out)


def solution(mesh):
    return jax.shard_map(
        body,
        mesh=mesh,
        in_specs=(
            P("ep", "tp"),
            P(("ep", "tp"), None),
            P(("ep", "tp"), None),
            P(),
            P(None, "tp"),
            P(None, "tp"),
            P(),
            P(("ep", "tp"), None),
            P(),
            P(("ep", "tp"), None),
            P(("ep", "tp")),
            P(("ep", "tp"), None),
            P("ep", None, "tp"),
            P("ep", None, "tp"),
            P("ep", "tp", None),
        ),
        out_specs=(P(("ep", "tp"), None), P(("ep", "tp"), None)),
        check_vma=False,
    )
```

```python
import math

import jax
import jax.numpy as jnp
import numpy as np
from jax import lax
from jax.experimental import pallas as pl
from jax.experimental.pallas import tpu as pltpu
from jax.sharding import PartitionSpec as P

NOPE = 64
ROPE_DIM = 32
MESH = pl.DeviceIdType.MESH

ZW = (1, 2, 3, 4)
SA = 6
SB = 9
SM = 1
SF = 11
LO = ((5, 0), (7, 2), (8, 4), (10, 6), (11, 7))
HI = ((5, 2), (7, 4), (8, 6), (10, 7), (11, 8))


epsilon = 1e-06
rope_base = 10000.0
masked_value = -1e30


def rotation(positions):
    inverse = rope_base ** (-2.0 * np.arange(ROPE_DIM // 2) / ROPE_DIM)
    angles = np.tile(positions[:, None] * inverse[None, :], (1, 2))
    return jnp.asarray(np.concatenate([np.cos(angles), np.sin(angles)], axis=1), jnp.float32)


def plain_copy(first, second):
    def kernel(a_ref, b_ref, c_ref, d_ref):
        c_ref[...] = a_ref[...]
        d_ref[...] = b_ref[...]

    vmem = pl.BlockSpec(memory_space=pltpu.VMEM)
    return pl.pallas_call(
        kernel,
        out_shape=(
            jax.ShapeDtypeStruct(first.shape, first.dtype),
            jax.ShapeDtypeStruct(second.shape, second.dtype),
        ),
        in_specs=[vmem, vmem],
        out_specs=(vmem, vmem),
        name="plain_copy",
    )(first, second)


def exchange(
    tokens, moe_gain, routes, group_prob, expert_prob, within, starts, latent, rope_key, latent_gain,
    query, w_gate, w_up, w_down, key_up, value_up, out_proj,
):
    width = tokens.shape[1] // 4
    units = w_gate.shape[1]
    ranks = lax.axis_size("ep")
    depth = ranks // 8
    f32, bf16 = jnp.float32, jnp.bfloat16
    shift = math.log2(math.e) / math.sqrt(NOPE + ROPE_DIM)

    def kernel(
        tok_hbm, gain_hbm, routes_hbm, group_hbm, prob_hbm, within_hbm, starts_hbm, lat_hbm, rope_hbm, lgain_hbm,
        q_hbm, wg_hbm, wu_hbm, wd_hbm, ku_hbm, vu_hbm, wp_hbm, mixed_ref, o_ref,
        gain_ref, routes_ref, group_ref, prob_ref, within_ref, starts_ref, lgain_ref, tok, lin, rin, qin, nx_ref, note_ref, lat_ref, q_ref, turn_ref,
        xn, note, slab, rows, wg, wu, wd, hid, back, ret, moved, final, mix,
        lat, ku, vu, wp, kv, top, total, acc, attm, attx,
        load_sem, own_sem, small_recv, arrive, ret_sem, ring_recv, send_sem, kv_recv, kv_send,
    ):
        me, t = lax.axis_index("ep"), lax.axis_index("tp")
        z = me // 8
        y, c = lax.rem(me, 8) // 2, lax.rem(me, 2)
        g0 = lax.rem(me, 8)
        right, left = lax.rem(t + 1, 4), lax.rem(t + 3, 4)

        loads = [
            pltpu.make_async_copy(wg_hbm, wg, load_sem.at[0]),
            pltpu.make_async_copy(wu_hbm, wu, load_sem.at[1]),
            pltpu.make_async_copy(wd_hbm.at[:, pl.ds(pl.multiple_of(t * width, width), width)], wd.at[t], load_sem.at[2]),
            pltpu.make_async_copy(wp_hbm, wp, load_sem.at[3]),
        ]
        early = [
            pltpu.make_async_copy(ku_hbm, ku, load_sem.at[4]),
            pltpu.make_async_copy(vu_hbm, vu, load_sem.at[5]),
        ]
        small_loads = [
            pltpu.make_async_copy(gain_hbm, gain_ref, load_sem.at[10]),
            pltpu.make_async_copy(routes_hbm, routes_ref, load_sem.at[11]),
            pltpu.make_async_copy(group_hbm, group_ref, load_sem.at[12]),
            pltpu.make_async_copy(prob_hbm, prob_ref, load_sem.at[13]),
            pltpu.make_async_copy(within_hbm, within_ref, load_sem.at[14]),
            pltpu.make_async_copy(starts_hbm, starts_ref, load_sem.at[15]),
            pltpu.make_async_copy(lgain_hbm, lgain_ref, load_sem.at[16]),
        ]
        first_loads = [
            pltpu.make_async_copy(tok_hbm, tok, load_sem.at[6]),
            pltpu.make_async_copy(lat_hbm, lin, load_sem.at[7]),
            pltpu.make_async_copy(rope_hbm, rin, load_sem.at[8]),
            pltpu.make_async_copy(q_hbm, qin, load_sem.at[9]),
        ]
        for load in small_loads + first_loads + early + loads:
            load.start()

        barrier = pltpu.get_barrier_semaphore()

        def greet(k, _):
            pl.semaphore_signal(barrier, inc=1, device_id=(lax.rem(me + k, ranks), t), device_id_type=MESH)
            return 0

        def greet_both(k, _):
            greet(ranks // 2 + k, 0)
            return greet(ranks // 2 - k, 0)

        greet(ranks // 2, 0)
        lax.fori_loop(1, ranks // 2, greet_both, 0)
        for k in range(1, 4):
            pl.semaphore_signal(barrier, inc=1, device_id=(me, lax.rem(t + k, 4)), device_id_type=MESH)

        def normed(ref, gain):
            wide = ref[...].astype(f32)
            return wide * lax.rsqrt(jnp.mean(wide * wide, axis=-1, keepdims=True) + epsilon) * gain[...]

        def turned(part, cosine, sine):
            half = ROPE_DIM // 2
            swapped = jnp.concatenate([part[:, half:], part[:, :half]], axis=1)
            return part * cosine + swapped * sine

        for load in small_loads:
            load.wait()
        choice = routes_ref[...].astype(f32)
        down_at = lax.broadcasted_iota(jnp.int32, (64, 64), 0)
        across_at = lax.broadcasted_iota(jnp.int32, (64, 64), 1)
        columns = [
            jnp.sum(jnp.where(down_at == across_at, choice[k : k + 1], 0.0), axis=1, keepdims=True) for k in range(2)
        ]
        odds = prob_ref[...]
        note_ref[...] = jnp.zeros(note_ref.shape, f32)
        for k in range(2):
            row = choice[k : k + 1]
            same = jnp.where(columns[0] == row, 1.0, 0.0) + jnp.where(columns[1] == row, 1.0, 0.0)
            slot = jnp.sum(jnp.where(down_at < across_at, same, 0.0), axis=0, keepdims=True)
            note_ref[k : k + 1, 0:64] = row * 16.0 + slot + (t * 4).astype(f32)
            note_ref[2 + k : 3 + k, 0:64] = group_ref[...] * odds[k : k + 1] / (odds[0:1] + odds[1:2])
        for load in first_loads:
            load.wait()
        nx_ref[...] = normed(tok, gain_ref).astype(bf16)
        lat_ref[:, : lin.shape[1]] = normed(lin, lgain_ref).astype(bf16)
        near, far = within_ref[...], starts_ref[pl.ds(me, 1)]
        near_cos, near_sin, far_cos, far_sin = near[:, :32], near[:, 32:], far[:, :32], far[:, 32:]
        sine = near_sin * far_cos + near_cos * far_sin
        lower = lax.broadcasted_iota(jnp.int32, sine.shape, 1) < ROPE_DIM // 2
        turn_ref[:, :32] = near_cos * far_cos - near_sin * far_sin
        turn_ref[:, 32:] = jnp.where(lower, -sine, sine)
        table = turn_ref[pl.ds(pl.multiple_of(t * 32, 32), 32)]
        own_key = turned(rin[...].astype(f32), table[:, :32], table[:, 32:])
        own_lanes = lax.broadcasted_iota(jnp.int32, (32, 128), 1) // 32 == t
        lat_ref[:, lin.shape[1] :] = jnp.where(own_lanes, jnp.concatenate([own_key] * 4, axis=1), 0.0).astype(bf16)
        pl.semaphore_wait(barrier, ranks + 2)

        def remote(s, d, send, recv, e, x):
            return pltpu.make_async_remote_copy(
                src_ref=s, dst_ref=d, send_sem=send, recv_sem=recv, device_id=(e, x), device_id_type=MESH
            )

        def cols(x):
            return pl.ds(pl.multiple_of(x * width, width), width)

        def small(k, kind):
            x = lax.rem(t + k, 4)
            send, recv = send_sem.at[6 + 3 * kind + k - 1], small_recv.at[kind, t]
            if kind == 0:
                return remote(nx_ref.at[:, cols(x)], xn.at[t], send, recv, me, x)
            if kind == 1:
                return remote(note_ref, note.at[t], send, recv, me, x)
            if kind == 3:
                return remote(wd_hbm.at[:, cols(x)], wd.at[t], send, recv, me, x)
            if kind == 4:
                return remote(moved.at[x], final.at[:, cols(t)], send, recv, me, x)
            if kind == 5:
                return remote(lat_ref, lat.at[t], send, recv, me, x)
            return remote(attm.at[x], attx.at[t], send, recv, me, x)

        def small_arrived(k, kind):
            x = lax.rem(t + k, 4)
            recv = small_recv.at[kind, x]
            ref = (xn.at[x], note.at[x], None, wd.at[x], final.at[:, cols(x)], lat.at[x], attx.at[x])[kind]
            return remote(ref, ref, send_sem.at[5], recv, me, x)

        for kind in (0, 1, 5, 3):
            for k in (2, 1, 3):
                small(k, kind).start()
        lat[t] = lat_ref[...]
        xn[t] = nx_ref[:, cols(t)]
        note[t] = note_ref[...]
        for kind in range(2):
            for k in range(1, 4):
                small_arrived(k, kind).wait_recv()

        notes = jnp.concatenate([note[x, :, 0:64] for x in range(4)], axis=1)
        first, second = notes[0:1].astype(jnp.int32), notes[1:2].astype(jnp.int32)
        tokens = xn[...].reshape(256, width)

        def offset(i):
            return jnp.where(i == 6, 7, jnp.where(i == 5, 1, jnp.where(i == 4, 5, jnp.where(i == 3, 3, jnp.where(i == 2, 4, jnp.where(i == 1, 6, jnp.where(i == 0, 2, jnp.int32(0))))))))

        def own_slab():
            return pltpu.make_async_copy(slab.at[me], rows.at[t, me], own_sem.at[0])

        def dispatch(i, _):
            zd = lax.rem(z + offset(i), depth)
            row = lax.broadcasted_iota(jnp.int32, (128, 256), 0) + zd * 128
            table = jnp.where((row == first) | (row == second), 1.0, 0.0).astype(bf16)
            out = jnp.dot(table, tokens, preferred_element_type=f32).astype(bf16)
            slab[pl.ds(zd * 8, 8)] = out.reshape(8, 16, width)

            def send(k, _):
                dst = zd * 8 + k

                @pl.when(dst != me)
                def _():
                    remote(slab.at[dst], rows.at[t, me], send_sem.at[0], arrive.at[me], dst, t).start()

                return 0

            lax.fori_loop(0, 8, send, 0)
            return 0

        def plane(dz):
            return lax.rem(z + dz + depth, depth)

        def column(dy, flip=0):
            return lax.rem(y + dy + 4, 4) * 2 + (c if flip == 0 else 1 - c)

        def along_z(d, step, arrived=False):
            sign = 1 if d == 0 else -1
            block = plane(-sign * (step if arrived else step - 1))
            ref = kv.at[g0, block] if step < 4 else kv.at[g0, block, pl.ds(272 * d, 272)]
            n = 4 * d + step - 1
            return remote(ref, ref, kv_send.at[n], kv_recv.at[n], plane(sign) * 8 + g0, t)

        def along_y(d, block, arrived=False):
            sign = 1 if d == 0 else -1
            ref = kv.at[column(-sign if arrived else 0), block]
            n = 8 + 8 * d + block
            return remote(ref, ref, kv_send.at[n], kv_recv.at[n], z * 8 + column(sign), t)

        def along_y2(d, arrived=False):
            sign = 1 if d == 0 else -1
            ref = kv.at[column(-sign * (2 if arrived else 1)), pl.ds(4 * d, 4)]
            return remote(ref, ref, kv_send.at[24 + d], kv_recv.at[24 + d], z * 8 + column(sign), t)

        def across(i, arrived=False):
            ref = kv.at[column((0, -1, 1, 2)[i], 1 if arrived else 0)]
            return remote(ref, ref, kv_send.at[26 + i], kv_recv.at[26 + i], z * 8 + column(0, 1), t)

        dispatch(0, 0)
        for k in range(1, 4):
            small_arrived(k, 5).wait_recv()
        for load in early:
            load.wait()
        flat = lat[...].reshape(128, lat.shape[2])
        latent = flat[:, : ku.shape[0]]
        keys = jnp.dot(latent, ku[...], preferred_element_type=f32).astype(bf16)
        values = jnp.dot(latent, vu[...], preferred_element_type=f32)
        kv[g0, z, 0:128] = keys[:, :128]
        kv[g0, z, 128:256] = keys[:, 128:]
        kv[g0, z, 256:512] = values.T.astype(bf16)
        packed = lat[0, :, ku.shape[0] :].astype(f32)
        for x in range(1, 4):
            packed = packed + lat[x, :, ku.shape[0] :].astype(f32)
        kv[g0, z, 512:544] = packed.astype(bf16)
        for d in range(2):
            along_z(d, 1).start()
            along_y(d, z).start()
        lax.fori_loop(1, depth, dispatch, 0)
        own_slab().start()
        q_ref[...] = jnp.zeros(q_ref.shape, bf16)
        asked = qin[...].astype(f32)
        for h in range(4):
            p, i = h // 2, h % 2
            nope = asked[:, 96 * h : 96 * h + 64].astype(bf16)
            rope = turned(asked[:, 96 * h + 64 : 96 * h + 96], turn_ref[:, :32], turn_ref[:, 32:]).astype(bf16)
            for j in range(4):
                q_ref[p, j, 128 * i : 128 * i + 128, 64 * i : 64 * i + 64] = nope
                q_ref[p, j, 128 * i : 128 * i + 128, 128 + 32 * j : 160 + 32 * j] = rope
        top[...] = jnp.full(top.shape, masked_value, f32)
        total[...] = jnp.zeros(total.shape, f32)
        acc[...] = jnp.zeros(acc.shape, f32)

        def attend(k, _):
            for i, at in enumerate((1, 4, 5, 7)):

                @pl.when(k == at)
                def _():
                    across(i, True).wait_recv()

            dy = jnp.where(k < 2, 0, jnp.where(k >= 6, 2, jnp.where(lax.rem(k, 2) == 0, 3, 1)))
            flip = (k == 1) | (k == 4) | (k == 5) | (k == 7)
            col = lax.rem(y + dy, 4) * 2 + jnp.where(flip, 1 - c, c)
            rope = kv[col, :, 512:544, :].reshape(256, 128)
            for p in range(2):
                parts = []
                for j in range(4):
                    some = kv[col, :, 128 * p + 32 * j : 128 * p + 32 * j + 32, :]
                    both = jnp.concatenate([some.reshape(256, 128), rope], axis=1)
                    s = lax.dot_general(both, q_ref[p, j], (((1,), (1,)), ((), ())), preferred_element_type=f32)
                    s = s.reshape(8, 32, 256)
                    place = lax.broadcasted_iota(jnp.int32, s.shape, 0) * 1024 + lax.broadcasted_iota(jnp.int32, s.shape, 1)
                    query = lax.broadcasted_iota(jnp.int32, s.shape, 2) & 127
                    parts.append(jnp.where(place - query <= (me - col) * 128 - 32 * j, s, masked_value))
                peak = parts[0].max(axis=0)
                for s in parts[1:]:
                    peak = jnp.maximum(peak, s.max(axis=0))
                before = top[p]
                peak = jnp.maximum(before, peak.max(axis=0, keepdims=True))
                factor = jnp.exp2((before - peak) * shift)
                added = jnp.zeros((32, 256), f32)
                raised = []
                for s in parts:
                    r = jnp.exp2((s - peak[None]) * shift)
                    added = added + r.sum(axis=0)
                    raised.append(r.astype(bf16))
                total[p] = total[p] * factor + added.sum(axis=0, keepdims=True)
                top[p] = peak
                weights = jnp.concatenate(raised, axis=1)
                update = acc[p] * factor
                for r in range(0, 8, 2):
                    vals = jnp.concatenate(
                        [kv[col, r + i, 256 + 128 * p : 384 + 128 * p, :] for i in range(2)], axis=1
                    )
                    update = update + jnp.dot(vals, weights[r : r + 2].reshape(256, 256), preferred_element_type=f32)
                acc[p] = update
            return 0

        def attended():
            pieces = []
            for p in range(2):
                a, l = acc[p], total[p]
                for i in range(2):
                    lanes = slice(128 * i, 128 * i + 128)
                    pieces.append(a[64 * i : 64 * i + 64, lanes] / l[:, lanes])
            attm[...] = jnp.concatenate(pieces, axis=0).T.astype(bf16).reshape(4, 32, 256)
            for k in (1, 3, 2):
                small(k, 6).start()
            attx[t] = attm[t]

        def ring(kind, chunk, block, d):
            buf = rows if kind < 2 else hid
            to = right if d == 0 else left
            origin = t if kind % 2 == 0 else (left if d == 0 else right)
            part = pl.ds(block * 8, 8) if kind % 2 == 0 else pl.ds(block * 8 + 4 * d, 4)
            ref = buf.at[origin, part]
            return remote(ref, ref, send_sem.at[1 + kind], ring_recv.at[kind, d, chunk], me, to)

        def ring_arrived(kind, chunk, block, d):
            buf = rows if kind < 2 else hid
            origin = (left if d == 0 else right) if kind % 2 == 0 else lax.rem(t + 2, 4)
            part = pl.ds(block * 8, 8) if kind % 2 == 0 else pl.ds(block * 8 + 4 * d, 4)
            ref = buf.at[origin, part]
            return remote(ref, ref, send_sem.at[5], ring_recv.at[kind, d, chunk], me, left)

        for load in loads:
            load.wait()

        def block_of(chunk):
            return lax.rem(z - offset(chunk) + depth, depth)

        def mix_tables():
            for n4 in range(4):
                row = lax.broadcasted_iota(jnp.int32, (ranks * 4, 256), 0) + n4 * ranks * 4
                table = jnp.where(row == first, notes[2:3], 0.0) + jnp.where(row == second, notes[3:4], 0.0)
                mix[:, n4 * ranks * 4 : (n4 + 1) * ranks * 4] = table.T.astype(bf16)

        def pick(s, table):
            out = jnp.int32(0)
            for at, value in table:
                out = jnp.where(s == at, value, out)
            return out

        def stage(s, _):
            @pl.when(s < depth)
            def _():
                block = block_of(s)

                def got(k, _):
                    e = block * 8 + k

                    @pl.when(e != me)
                    def _():
                        remote(rows.at[t, e], rows.at[t, e], send_sem.at[5], arrive.at[e], e, t).wait_recv()

                    @pl.when(e == me)
                    def _():
                        own_slab().wait()

                    return 0

                lax.fori_loop(0, 8, got, 0)
                for d in range(2):
                    ring(0, s, block, d).start()

            @pl.when((s >= 1) & (s < depth + 1))
            def _():
                block = block_of(s - 1)
                for d in range(2):
                    ring_arrived(0, s - 1, block, d).wait_recv()
                    ring(1, s - 1, block, d).start()

            @pl.when((s >= 2) & (s < depth + 2))
            def _():
                block = block_of(s - 2)
                for d in range(2):
                    ring_arrived(1, s - 2, block, d).wait_recv()
                gate = jnp.zeros((128, units), f32)
                up = jnp.zeros((128, units), f32)
                for x in range(4):
                    part = rows[x, pl.ds(block * 8, 8)].reshape(128, width)
                    gate = gate + jnp.dot(part, wg[width * x : width * x + width], preferred_element_type=f32)
                    up = up + jnp.dot(part, wu[width * x : width * x + width], preferred_element_type=f32)
                hidden = (gate / (1.0 + jnp.exp(-gate)) * up).astype(bf16)
                hid[t, pl.ds(block * 8, 8)] = hidden.reshape(8, 16, units)
                for d in range(2):
                    ring(2, s - 2, block, d).start()

            @pl.when((s >= 3) & (s < depth + 3))
            def _():
                block = block_of(s - 3)
                for d in range(2):
                    ring_arrived(2, s - 3, block, d).wait_recv()
                    ring(3, s - 3, block, d).start()

            @pl.when(s == 4)
            def _():
                for k in range(1, 4):
                    small_arrived(k, 3).wait_recv()

            @pl.when(s >= 4)
            def _():
                block = block_of(s - 4)
                for d in range(2):
                    ring_arrived(3, s - 4, block, d).wait_recv()
                total = jnp.zeros((128, width), f32)
                for x in range(4):
                    part = hid[x, pl.ds(block * 8, 8)].reshape(128, units)
                    total = total + jnp.dot(part, wd[x], preferred_element_type=f32).astype(bf16).astype(f32)
                back[pl.ds(block * 8, 8)] = total.astype(bf16).reshape(8, 16, width)

                def send(k, _):
                    e = block * 8 + k

                    @pl.when(e != me)
                    def _():
                        remote(back.at[e], ret.at[me], send_sem.at[27], ret_sem.at[me], e, t).start()

                    return 0

                lax.fori_loop(0, 8, send, 0)

            for step in range(1, 5):

                @pl.when(s == ZW[step - 1])
                def _(step=step):
                    for d in range(2):
                        along_z(d, step, True).wait_recv()
                        if step < 4:
                            along_z(d, step + 1).start()
                    for block in (plane(-step), plane(step)) if step < 4 else (plane(4),):
                        for d in range(2):
                            along_y(d, block).start()
                    if step == 4:
                        across(0).start()

            @pl.when(s == SA)
            def _():
                for d in range(2):
                    lax.fori_loop(0, depth, lambda b, _, d=d: (along_y(d, b, True).wait_recv(), 0)[1], 0)
                    along_y2(d).start()
                    across(1 + d).start()

            @pl.when(s == SB)
            def _():
                for d in range(2):
                    along_y2(d, True).wait_recv()
                across(3).start()

            @pl.when(s == SM)
            def _():
                mix_tables()

            lax.fori_loop(pick(s, LO), pick(s, HI), attend, 0)

            @pl.when(s == SF)
            def _():
                attended()

            return 0

        lax.fori_loop(0, depth + 4, stage, 0)

        ret[me] = back[me]

        def came(e, _):
            @pl.when(e != me)
            def _():
                remote(ret.at[e], ret.at[e], send_sem.at[5], ret_sem.at[e], e, t).wait_recv()

            return 0

        lax.fori_loop(0, ranks, came, 0)
        given = ret[...].reshape(ranks * 16, width)
        summed = jnp.dot(mix[...], given, preferred_element_type=f32)
        moved[...] = summed.astype(bf16).reshape(4, 64, width)
        for k in (1, 3, 2):
            small(k, 4).start()
        final[:, cols(t)] = moved[t]
        for k in range(1, 4):
            small_arrived(k, 6).wait_recv()
        for n in range(4):
            at = slice(n * width, n * width + width)
            out = jnp.zeros((32, width), f32)
            for x in range(4):
                out = out + jnp.dot(attx[x], wp[256 * x : 256 * x + 256, at], preferred_element_type=f32)
            mixed_ref[:, at] = out.astype(bf16)
        for k in range(1, 4):
            small_arrived(k, 4).wait_recv()
        o_ref[...] = final[...]

        def drain(ref, sem):
            remote(ref, ref, sem, arrive.at[0], me, left).wait_send()

        drain(slab.at[pl.ds(0, ranks - 1)], send_sem.at[0])
        drain(rows.at[pl.ds(0, 2)], send_sem.at[1])
        drain(rows.at[0], send_sem.at[2])
        drain(hid.at[pl.ds(0, 2)], send_sem.at[3])
        drain(hid.at[0], send_sem.at[4])
        drain(back.at[pl.ds(0, ranks - 1)], send_sem.at[27])
        for kind in (0, 1, 3, 4, 5, 6):
            for k in range(1, 4):
                small(k, kind).wait_send()
        for d in range(2):
            for step in range(1, 5):
                along_z(d, step).wait_send()
            lax.fori_loop(0, depth, lambda b, _, d=d: (along_y(d, b).wait_send(), 0)[1], 0)
            along_y2(d).wait_send()
        for i in range(4):
            across(i).wait_send()

    vmem = pl.BlockSpec(memory_space=pltpu.VMEM)
    hbm = pl.BlockSpec(memory_space=pl.ANY)
    return pl.pallas_call(
        kernel,
        out_shape=(jax.ShapeDtypeStruct((32, tokens.shape[1]), bf16), jax.ShapeDtypeStruct(tokens.shape, bf16)),
        in_specs=[hbm] * 17,
        out_specs=(vmem, vmem),
        scratch_shapes=[
            pltpu.VMEM(moe_gain.shape, moe_gain.dtype),
            pltpu.VMEM(routes.shape, routes.dtype),
            pltpu.VMEM(group_prob.shape, group_prob.dtype),
            pltpu.VMEM(expert_prob.shape, expert_prob.dtype),
            pltpu.VMEM(within.shape, within.dtype),
            pltpu.VMEM(starts.shape, starts.dtype),
            pltpu.VMEM(latent_gain.shape, latent_gain.dtype),
            pltpu.VMEM(tokens.shape, bf16),
            pltpu.VMEM(latent.shape, bf16),
            pltpu.VMEM(rope_key.shape, bf16),
            pltpu.VMEM(query.shape, bf16),
            pltpu.VMEM(tokens.shape, bf16),
            pltpu.VMEM((8, 128), f32),
            pltpu.VMEM((32, latent.shape[1] + 128), bf16),
            pltpu.VMEM((2, 4, 256, 256), bf16),
            pltpu.VMEM((128, 64), f32),
            pltpu.VMEM((4, 64, width), bf16),
            pltpu.VMEM((4, 8, 128), f32),
            pltpu.VMEM((ranks, 16, width), bf16),
            pltpu.VMEM((4, ranks, 16, width), bf16),
            pltpu.VMEM(w_gate.shape, bf16),
            pltpu.VMEM(w_up.shape, bf16),
            pltpu.VMEM((4, units, width), bf16),
            pltpu.VMEM((4, ranks, 16, units), bf16),
            pltpu.VMEM((ranks, 16, width), bf16),
            pltpu.VMEM((ranks, 16, width), bf16),
            pltpu.VMEM((4, 64, width), bf16),
            pltpu.VMEM(tokens.shape, bf16),
            pltpu.VMEM((256, ranks * 16), bf16),
            pltpu.VMEM((4, 32, latent.shape[1] + 128), bf16),
            pltpu.VMEM(key_up.shape, bf16),
            pltpu.VMEM(value_up.shape, bf16),
            pltpu.VMEM(out_proj.shape, bf16),
            pltpu.VMEM((8, depth, 544, 128), bf16),
            pltpu.VMEM((2, 1, 256), f32),
            pltpu.VMEM((2, 1, 256), f32),
            pltpu.VMEM((2, 128, 256), f32),
            pltpu.VMEM((4, 32, 256), bf16),
            pltpu.VMEM((4, 32, 256), bf16),
            pltpu.SemaphoreType.DMA((17,)),
            pltpu.SemaphoreType.DMA((1,)),
            pltpu.SemaphoreType.DMA((7, 4)),
            pltpu.SemaphoreType.DMA((ranks,)),
            pltpu.SemaphoreType.DMA((ranks,)),
            pltpu.SemaphoreType.DMA((4, 2, 8)),
            pltpu.SemaphoreType.DMA((28,)),
            pltpu.SemaphoreType.DMA((30,)),
            pltpu.SemaphoreType.DMA((30,)),
        ],
        compiler_params=pltpu.CompilerParams(
            collective_id=0, has_side_effects=True, vmem_limit_bytes=56 << 20
        ),
        cost_estimate=pl.CostEstimate(flops=5 * 10**9, bytes_accessed=3 * 10**7, transcendentals=0),
        name="exchange",
    )(
        tokens, moe_gain, routes, group_prob, expert_prob, within, starts, latent, rope_key, latent_gain,
        query, w_gate, w_up, w_down, key_up, value_up, out_proj,
    )


def body(
    query,
    latent,
    rope_key,
    latent_gain,
    key_up,
    value_up,
    out_proj,
    tokens,
    moe_gain,
    routes,
    group_prob,
    expert_prob,
    w_gate,
    w_up,
    w_down,
):
    rows = query.shape[0]
    within, starts = rotation(np.arange(rows)), rotation(np.arange(lax.axis_size("ep")) * rows)
    mixed, moe_out = exchange(
        tokens, moe_gain[None], routes.T, group_prob[None], expert_prob.T, within, starts, latent, rope_key, latent_gain[None],
        query, w_gate[0], w_up[0], w_down[0], key_up, value_up, out_proj,
    )
    return plain_copy(mixed, moe_out)


def solution(mesh):
    return jax.shard_map(
        body,
        mesh=mesh,
        in_specs=(
            P("ep", "tp"),
            P(("ep", "tp"), None),
            P(("ep", "tp"), None),
            P(),
            P(None, "tp"),
            P(None, "tp"),
            P(),
            P(("ep", "tp"), None),
            P(),
            P(("ep", "tp"), None),
            P(("ep", "tp")),
            P(("ep", "tp"), None),
            P("ep", None, "tp"),
            P("ep", None, "tp"),
            P("ep", "tp", None),
        ),
        out_specs=(P(("ep", "tp"), None), P(("ep", "tp"), None)),
        check_vma=False,
    )
```

```python
import math

import jax
import jax.numpy as jnp
import numpy as np
from jax import lax
from jax.experimental import pallas as pl
from jax.experimental.pallas import tpu as pltpu
from jax.sharding import PartitionSpec as P

NOPE = 64
ROPE_DIM = 32
MESH = pl.DeviceIdType.MESH

ZW = (1, 2, 3, 4)
SA = 6
SB = 9
SM = 1
SF = 11
LO = ((5, 0), (7, 2), (8, 4), (10, 6), (11, 7))
HI = ((5, 2), (7, 4), (8, 6), (10, 7), (11, 8))


epsilon = 1e-06
rope_base = 10000.0
masked_value = -1e30


def rotation(positions):
    inverse = rope_base ** (-2.0 * np.arange(ROPE_DIM // 2) / ROPE_DIM)
    angles = np.tile(positions[:, None] * inverse[None, :], (1, 2))
    return jnp.asarray(np.concatenate([np.cos(angles), np.sin(angles)], axis=1), jnp.float32)


def plain_copy(first, second):
    half = second.shape[0] // 2

    def kernel(a_ref, b_ref, c_ref, d_ref, held_a, held_b, load_sem, store_sem):
        parts = (
            (a_ref, held_a, c_ref),
            (b_ref.at[:half], held_b.at[:half], d_ref.at[:half]),
            (b_ref.at[half:], held_b.at[half:], d_ref.at[half:]),
        )
        loads = [pltpu.make_async_copy(p[0], p[1], load_sem.at[n]) for n, p in enumerate(parts)]
        stores = [pltpu.make_async_copy(p[1], p[2], store_sem.at[n]) for n, p in enumerate(parts)]
        for load in loads:
            load.start()
        for load, store in zip(loads, stores):
            load.wait()
            store.start()
        for store in stores:
            store.wait()

    anywhere = pl.BlockSpec(memory_space=pl.ANY)
    return pl.pallas_call(
        kernel,
        out_shape=(
            jax.ShapeDtypeStruct(first.shape, first.dtype),
            jax.ShapeDtypeStruct(second.shape, second.dtype),
        ),
        in_specs=[anywhere, anywhere],
        out_specs=(anywhere, anywhere),
        scratch_shapes=[
            pltpu.VMEM(first.shape, first.dtype),
            pltpu.VMEM(second.shape, second.dtype),
            pltpu.SemaphoreType.DMA((3,)),
            pltpu.SemaphoreType.DMA((3,)),
        ],
        name="plain_copy",
    )(first, second)


def exchange(
    tokens, moe_gain, routes, group_prob, expert_prob, within, starts, latent, rope_key, latent_gain,
    query, w_gate, w_up, w_down, key_up, value_up, out_proj,
):
    width = tokens.shape[1] // 4
    units = w_gate.shape[1]
    ranks = lax.axis_size("ep")
    depth = ranks // 8
    f32, bf16 = jnp.float32, jnp.bfloat16
    shift = math.log2(math.e) / math.sqrt(NOPE + ROPE_DIM)

    def kernel(
        tok_hbm, gain_hbm, routes_hbm, group_hbm, prob_hbm, within_hbm, starts_hbm, lat_hbm, rope_hbm, lgain_hbm,
        q_hbm, wg_hbm, wu_hbm, wd_hbm, ku_hbm, vu_hbm, wp_hbm, mixed_ref, o_ref,
        gain_ref, routes_ref, group_ref, prob_ref, within_ref, starts_ref, lgain_ref, tok, lin, rin, qin, nx_ref, note_ref, lat_ref, q_ref, turn_ref,
        xn, note, slab, rows, wg, wu, wd, hid, back, ret, moved, final, mix,
        lat, ku, vu, wp, kv, top, total, acc, attm, attx,
        load_sem, own_sem, small_recv, arrive, ret_sem, ring_recv, send_sem, kv_recv, kv_send,
    ):
        me, t = lax.axis_index("ep"), lax.axis_index("tp")
        z = me // 8
        y, c = lax.rem(me, 8) // 2, lax.rem(me, 2)
        g0 = lax.rem(me, 8)
        right, left = lax.rem(t + 1, 4), lax.rem(t + 3, 4)

        loads = [
            pltpu.make_async_copy(wg_hbm, wg, load_sem.at[0]),
            pltpu.make_async_copy(wu_hbm, wu, load_sem.at[1]),
            pltpu.make_async_copy(wd_hbm.at[:, pl.ds(pl.multiple_of(t * width, width), width)], wd.at[t], load_sem.at[2]),
            pltpu.make_async_copy(wp_hbm, wp, load_sem.at[3]),
        ]
        early = [
            pltpu.make_async_copy(ku_hbm, ku, load_sem.at[4]),
            pltpu.make_async_copy(vu_hbm, vu, load_sem.at[5]),
        ]
        small_loads = [
            pltpu.make_async_copy(gain_hbm, gain_ref, load_sem.at[10]),
            pltpu.make_async_copy(routes_hbm, routes_ref, load_sem.at[11]),
            pltpu.make_async_copy(group_hbm, group_ref, load_sem.at[12]),
            pltpu.make_async_copy(prob_hbm, prob_ref, load_sem.at[13]),
            pltpu.make_async_copy(within_hbm, within_ref, load_sem.at[14]),
            pltpu.make_async_copy(starts_hbm, starts_ref, load_sem.at[15]),
            pltpu.make_async_copy(lgain_hbm, lgain_ref, load_sem.at[16]),
        ]
        first_loads = [
            pltpu.make_async_copy(tok_hbm, tok, load_sem.at[6]),
            pltpu.make_async_copy(lat_hbm, lin, load_sem.at[7]),
            pltpu.make_async_copy(rope_hbm, rin, load_sem.at[8]),
            pltpu.make_async_copy(q_hbm, qin, load_sem.at[9]),
        ]
        for load in small_loads + first_loads + early + loads:
            load.start()

        barrier = pltpu.get_barrier_semaphore()

        def greet(k, _):
            pl.semaphore_signal(barrier, inc=1, device_id=(lax.rem(me + k, ranks), t), device_id_type=MESH)
            return 0

        def greet_both(k, _):
            greet(ranks // 2 + k, 0)
            return greet(ranks // 2 - k, 0)

        greet(ranks // 2, 0)
        lax.fori_loop(1, ranks // 2, greet_both, 0)
        for k in range(1, 4):
            pl.semaphore_signal(barrier, inc=1, device_id=(me, lax.rem(t + k, 4)), device_id_type=MESH)

        def normed(ref, gain):
            wide = ref[...].astype(f32)
            return wide * lax.rsqrt(jnp.mean(wide * wide, axis=-1, keepdims=True) + epsilon) * gain[...]

        def turned(part, cosine, sine):
            half = ROPE_DIM // 2
            swapped = jnp.concatenate([part[:, half:], part[:, :half]], axis=1)
            return part * cosine + swapped * sine

        for load in small_loads:
            load.wait()
        choice = routes_ref[...].astype(f32)
        down_at = lax.broadcasted_iota(jnp.int32, (64, 64), 0)
        across_at = lax.broadcasted_iota(jnp.int32, (64, 64), 1)
        columns = [
            jnp.sum(jnp.where(down_at == across_at, choice[k : k + 1], 0.0), axis=1, keepdims=True) for k in range(2)
        ]
        odds = prob_ref[...]
        note_ref[...] = jnp.zeros(note_ref.shape, f32)
        for k in range(2):
            row = choice[k : k + 1]
            same = jnp.where(columns[0] == row, 1.0, 0.0) + jnp.where(columns[1] == row, 1.0, 0.0)
            slot = jnp.sum(jnp.where(down_at < across_at, same, 0.0), axis=0, keepdims=True)
            note_ref[k : k + 1, 0:64] = row * 16.0 + slot + (t * 4).astype(f32)
            note_ref[2 + k : 3 + k, 0:64] = group_ref[...] * odds[k : k + 1] / (odds[0:1] + odds[1:2])
        for load in first_loads:
            load.wait()
        nx_ref[...] = normed(tok, gain_ref).astype(bf16)
        lat_ref[:, : lin.shape[1]] = normed(lin, lgain_ref).astype(bf16)
        near, far = within_ref[...], starts_ref[pl.ds(me, 1)]
        near_cos, near_sin, far_cos, far_sin = near[:, :32], near[:, 32:], far[:, :32], far[:, 32:]
        sine = near_sin * far_cos + near_cos * far_sin
        lower = lax.broadcasted_iota(jnp.int32, sine.shape, 1) < ROPE_DIM // 2
        turn_ref[:, :32] = near_cos * far_cos - near_sin * far_sin
        turn_ref[:, 32:] = jnp.where(lower, -sine, sine)
        table = turn_ref[pl.ds(pl.multiple_of(t * 32, 32), 32)]
        own_key = turned(rin[...].astype(f32), table[:, :32], table[:, 32:])
        own_lanes = lax.broadcasted_iota(jnp.int32, (32, 128), 1) // 32 == t
        lat_ref[:, lin.shape[1] :] = jnp.where(own_lanes, jnp.concatenate([own_key] * 4, axis=1), 0.0).astype(bf16)
        pl.semaphore_wait(barrier, ranks + 2)

        def remote(s, d, send, recv, e, x):
            return pltpu.make_async_remote_copy(
                src_ref=s, dst_ref=d, send_sem=send, recv_sem=recv, device_id=(e, x), device_id_type=MESH
            )

        def cols(x):
            return pl.ds(pl.multiple_of(x * width, width), width)

        def small(k, kind):
            x = lax.rem(t + k, 4)
            send, recv = send_sem.at[6 + 3 * kind + k - 1], small_recv.at[kind, t]
            if kind == 0:
                return remote(nx_ref.at[:, cols(x)], xn.at[t], send, recv, me, x)
            if kind == 1:
                return remote(note_ref, note.at[t], send, recv, me, x)
            if kind == 3:
                return remote(wd_hbm.at[:, cols(x)], wd.at[t], send, recv, me, x)
            if kind == 4:
                return remote(moved.at[x], final.at[:, cols(t)], send, recv, me, x)
            if kind == 5:
                return remote(lat_ref, lat.at[t], send, recv, me, x)
            return remote(attm.at[x], attx.at[t], send, recv, me, x)

        def small_arrived(k, kind):
            x = lax.rem(t + k, 4)
            recv = small_recv.at[kind, x]
            ref = (xn.at[x], note.at[x], None, wd.at[x], final.at[:, cols(x)], lat.at[x], attx.at[x])[kind]
            return remote(ref, ref, send_sem.at[5], recv, me, x)

        for kind in (0, 1, 5, 3):
            for k in (2, 1, 3):
                small(k, kind).start()
        lat[t] = lat_ref[...]
        xn[t] = nx_ref[:, cols(t)]
        note[t] = note_ref[...]
        for kind in range(2):
            for k in range(1, 4):
                small_arrived(k, kind).wait_recv()

        notes = jnp.concatenate([note[x, :, 0:64] for x in range(4)], axis=1)
        first, second = notes[0:1].astype(jnp.int32), notes[1:2].astype(jnp.int32)
        tokens = xn[...].reshape(256, width)

        def offset(i):
            return jnp.where(i == 6, 7, jnp.where(i == 5, 1, jnp.where(i == 4, 5, jnp.where(i == 3, 3, jnp.where(i == 2, 4, jnp.where(i == 1, 6, jnp.where(i == 0, 2, jnp.int32(0))))))))

        def own_slab():
            return pltpu.make_async_copy(slab.at[me], rows.at[t, me], own_sem.at[0])

        def dispatch(i, _):
            zd = lax.rem(z + offset(i), depth)
            row = lax.broadcasted_iota(jnp.int32, (128, 256), 0) + zd * 128
            table = jnp.where((row == first) | (row == second), 1.0, 0.0).astype(bf16)
            out = jnp.dot(table, tokens, preferred_element_type=f32).astype(bf16)
            slab[pl.ds(zd * 8, 8)] = out.reshape(8, 16, width)

            def send(k, _):
                dst = zd * 8 + k

                @pl.when(dst != me)
                def _():
                    remote(slab.at[dst], rows.at[t, me], send_sem.at[0], arrive.at[me], dst, t).start()

                return 0

            lax.fori_loop(0, 8, send, 0)
            return 0

        def plane(dz):
            return lax.rem(z + dz + depth, depth)

        def column(dy, flip=0):
            return lax.rem(y + dy + 4, 4) * 2 + (c if flip == 0 else 1 - c)

        def along_z(d, step, arrived=False):
            sign = 1 if d == 0 else -1
            block = plane(-sign * (step if arrived else step - 1))
            ref = kv.at[g0, block] if step < 4 else kv.at[g0, block, pl.ds(272 * d, 272)]
            n = 4 * d + step - 1
            return remote(ref, ref, kv_send.at[n], kv_recv.at[n], plane(sign) * 8 + g0, t)

        def along_y(d, block, arrived=False):
            sign = 1 if d == 0 else -1
            ref = kv.at[column(-sign if arrived else 0), block]
            n = 8 + 8 * d + block
            return remote(ref, ref, kv_send.at[n], kv_recv.at[n], z * 8 + column(sign), t)

        def along_y2(d, arrived=False):
            sign = 1 if d == 0 else -1
            ref = kv.at[column(-sign * (2 if arrived else 1)), pl.ds(4 * d, 4)]
            return remote(ref, ref, kv_send.at[24 + d], kv_recv.at[24 + d], z * 8 + column(sign), t)

        def across(i, arrived=False):
            ref = kv.at[column((0, -1, 1, 2)[i], 1 if arrived else 0)]
            return remote(ref, ref, kv_send.at[26 + i], kv_recv.at[26 + i], z * 8 + column(0, 1), t)

        dispatch(0, 0)
        for k in range(1, 4):
            small_arrived(k, 5).wait_recv()
        for load in early:
            load.wait()
        flat = lat[...].reshape(128, lat.shape[2])
        latent = flat[:, : ku.shape[0]]
        keys = jnp.dot(latent, ku[...], preferred_element_type=f32).astype(bf16)
        values = jnp.dot(latent, vu[...], preferred_element_type=f32)
        kv[g0, z, 0:128] = keys[:, :128]
        kv[g0, z, 128:256] = keys[:, 128:]
        kv[g0, z, 256:512] = values.T.astype(bf16)
        packed = lat[0, :, ku.shape[0] :].astype(f32)
        for x in range(1, 4):
            packed = packed + lat[x, :, ku.shape[0] :].astype(f32)
        kv[g0, z, 512:544] = packed.astype(bf16)
        for d in range(2):
            along_z(d, 1).start()
            along_y(d, z).start()
        lax.fori_loop(1, depth, dispatch, 0)
        own_slab().start()
        q_ref[...] = jnp.zeros(q_ref.shape, bf16)
        asked = qin[...].astype(f32)
        for h in range(4):
            p, i = h // 2, h % 2
            nope = asked[:, 96 * h : 96 * h + 64].astype(bf16)
            rope = turned(asked[:, 96 * h + 64 : 96 * h + 96], turn_ref[:, :32], turn_ref[:, 32:]).astype(bf16)
            for j in range(4):
                q_ref[p, j, 128 * i : 128 * i + 128, 64 * i : 64 * i + 64] = nope
                q_ref[p, j, 128 * i : 128 * i + 128, 128 + 32 * j : 160 + 32 * j] = rope
        top[...] = jnp.full(top.shape, masked_value, f32)
        total[...] = jnp.zeros(total.shape, f32)
        acc[...] = jnp.zeros(acc.shape, f32)

        def attend(k, _):
            for i, at in enumerate((1, 4, 5, 7)):

                @pl.when(k == at)
                def _():
                    across(i, True).wait_recv()

            dy = jnp.where(k < 2, 0, jnp.where(k >= 6, 2, jnp.where(lax.rem(k, 2) == 0, 3, 1)))
            flip = (k == 1) | (k == 4) | (k == 5) | (k == 7)
            col = lax.rem(y + dy, 4) * 2 + jnp.where(flip, 1 - c, c)
            rope = kv[col, :, 512:544, :].reshape(256, 128)
            for p in range(2):
                parts = []
                for j in range(4):
                    some = kv[col, :, 128 * p + 32 * j : 128 * p + 32 * j + 32, :]
                    both = jnp.concatenate([some.reshape(256, 128), rope], axis=1)
                    s = lax.dot_general(both, q_ref[p, j], (((1,), (1,)), ((), ())), preferred_element_type=f32)
                    s = s.reshape(8, 32, 256)
                    place = lax.broadcasted_iota(jnp.int32, s.shape, 0) * 1024 + lax.broadcasted_iota(jnp.int32, s.shape, 1)
                    query = lax.broadcasted_iota(jnp.int32, s.shape, 2) & 127
                    parts.append(jnp.where(place - query <= (me - col) * 128 - 32 * j, s, masked_value))
                peak = parts[0].max(axis=0)
                for s in parts[1:]:
                    peak = jnp.maximum(peak, s.max(axis=0))
                before = top[p]
                peak = jnp.maximum(before, peak.max(axis=0, keepdims=True))
                factor = jnp.exp2((before - peak) * shift)
                added = jnp.zeros((32, 256), f32)
                raised = []
                for s in parts:
                    r = jnp.exp2((s - peak[None]) * shift)
                    added = added + r.sum(axis=0)
                    raised.append(r.astype(bf16))
                total[p] = total[p] * factor + added.sum(axis=0, keepdims=True)
                top[p] = peak
                weights = jnp.concatenate(raised, axis=1)
                update = acc[p] * factor
                for r in range(0, 8, 2):
                    vals = jnp.concatenate(
                        [kv[col, r + i, 256 + 128 * p : 384 + 128 * p, :] for i in range(2)], axis=1
                    )
                    update = update + jnp.dot(vals, weights[r : r + 2].reshape(256, 256), preferred_element_type=f32)
                acc[p] = update
            return 0

        def attended():
            pieces = []
            for p in range(2):
                a, l = acc[p], total[p]
                for i in range(2):
                    lanes = slice(128 * i, 128 * i + 128)
                    pieces.append(a[64 * i : 64 * i + 64, lanes] / l[:, lanes])
            attm[...] = jnp.concatenate(pieces, axis=0).T.astype(bf16).reshape(4, 32, 256)
            for k in (1, 3, 2):
                small(k, 6).start()
            attx[t] = attm[t]

        def ring(kind, chunk, block, d):
            buf = rows if kind < 2 else hid
            to = right if d == 0 else left
            origin = t if kind % 2 == 0 else (left if d == 0 else right)
            part = pl.ds(block * 8, 8) if kind % 2 == 0 else pl.ds(block * 8 + 4 * d, 4)
            ref = buf.at[origin, part]
            return remote(ref, ref, send_sem.at[1 + kind], ring_recv.at[kind, d, chunk], me, to)

        def ring_arrived(kind, chunk, block, d):
            buf = rows if kind < 2 else hid
            origin = (left if d == 0 else right) if kind % 2 == 0 else lax.rem(t + 2, 4)
            part = pl.ds(block * 8, 8) if kind % 2 == 0 else pl.ds(block * 8 + 4 * d, 4)
            ref = buf.at[origin, part]
            return remote(ref, ref, send_sem.at[5], ring_recv.at[kind, d, chunk], me, left)

        for load in loads:
            load.wait()

        def block_of(chunk):
            return lax.rem(z - offset(chunk) + depth, depth)

        def mix_tables():
            for n4 in range(4):
                row = lax.broadcasted_iota(jnp.int32, (ranks * 4, 256), 0) + n4 * ranks * 4
                table = jnp.where(row == first, notes[2:3], 0.0) + jnp.where(row == second, notes[3:4], 0.0)
                mix[:, n4 * ranks * 4 : (n4 + 1) * ranks * 4] = table.T.astype(bf16)

        def pick(s, table):
            out = jnp.int32(0)
            for at, value in table:
                out = jnp.where(s == at, value, out)
            return out

        def stage(s, _):
            @pl.when(s < depth)
            def _():
                block = block_of(s)

                def got(k, _):
                    e = block * 8 + k

                    @pl.when(e != me)
                    def _():
                        remote(rows.at[t, e], rows.at[t, e], send_sem.at[5], arrive.at[e], e, t).wait_recv()

                    @pl.when(e == me)
                    def _():
                        own_slab().wait()

                    return 0

                lax.fori_loop(0, 8, got, 0)
                for d in range(2):
                    ring(0, s, block, d).start()

            @pl.when((s >= 1) & (s < depth + 1))
            def _():
                block = block_of(s - 1)
                for d in range(2):
                    ring_arrived(0, s - 1, block, d).wait_recv()
                    ring(1, s - 1, block, d).start()

            @pl.when((s >= 2) & (s < depth + 2))
            def _():
                block = block_of(s - 2)
                for d in range(2):
                    ring_arrived(1, s - 2, block, d).wait_recv()
                gate = jnp.zeros((128, units), f32)
                up = jnp.zeros((128, units), f32)
                for x in range(4):
                    part = rows[x, pl.ds(block * 8, 8)].reshape(128, width)
                    gate = gate + jnp.dot(part, wg[width * x : width * x + width], preferred_element_type=f32)
                    up = up + jnp.dot(part, wu[width * x : width * x + width], preferred_element_type=f32)
                hidden = (gate / (1.0 + jnp.exp(-gate)) * up).astype(bf16)
                hid[t, pl.ds(block * 8, 8)] = hidden.reshape(8, 16, units)
                for d in range(2):
                    ring(2, s - 2, block, d).start()

            @pl.when((s >= 3) & (s < depth + 3))
            def _():
                block = block_of(s - 3)
                for d in range(2):
                    ring_arrived(2, s - 3, block, d).wait_recv()
                    ring(3, s - 3, block, d).start()

            @pl.when(s == 4)
            def _():
                for k in range(1, 4):
                    small_arrived(k, 3).wait_recv()

            @pl.when(s >= 4)
            def _():
                block = block_of(s - 4)
                for d in range(2):
                    ring_arrived(3, s - 4, block, d).wait_recv()
                total = jnp.zeros((128, width), f32)
                for x in range(4):
                    part = hid[x, pl.ds(block * 8, 8)].reshape(128, units)
                    total = total + jnp.dot(part, wd[x], preferred_element_type=f32).astype(bf16).astype(f32)
                back[pl.ds(block * 8, 8)] = total.astype(bf16).reshape(8, 16, width)

                def send(k, _):
                    e = block * 8 + k

                    @pl.when(e != me)
                    def _():
                        remote(back.at[e], ret.at[me], send_sem.at[27], ret_sem.at[me], e, t).start()

                    return 0

                lax.fori_loop(0, 8, send, 0)

            for step in range(1, 5):

                @pl.when(s == ZW[step - 1])
                def _(step=step):
                    for d in range(2):
                        along_z(d, step, True).wait_recv()
                        if step < 4:
                            along_z(d, step + 1).start()
                    for block in (plane(-step), plane(step)) if step < 4 else (plane(4),):
                        for d in range(2):
                            along_y(d, block).start()
                    if step == 4:
                        across(0).start()

            @pl.when(s == SA)
            def _():
                for d in range(2):
                    lax.fori_loop(0, depth, lambda b, _, d=d: (along_y(d, b, True).wait_recv(), 0)[1], 0)
                    along_y2(d).start()
                    across(1 + d).start()

            @pl.when(s == SB)
            def _():
                for d in range(2):
                    along_y2(d, True).wait_recv()
                across(3).start()

            @pl.when(s == SM)
            def _():
                mix_tables()

            lax.fori_loop(pick(s, LO), pick(s, HI), attend, 0)

            @pl.when(s == SF)
            def _():
                attended()

            return 0

        lax.fori_loop(0, depth + 4, stage, 0)

        ret[me] = back[me]

        def came(e, _):
            @pl.when(e != me)
            def _():
                remote(ret.at[e], ret.at[e], send_sem.at[5], ret_sem.at[e], e, t).wait_recv()

            return 0

        lax.fori_loop(0, ranks, came, 0)
        given = ret[...].reshape(ranks * 16, width)
        summed = jnp.dot(mix[...], given, preferred_element_type=f32)
        moved[...] = summed.astype(bf16).reshape(4, 64, width)
        for k in (1, 3, 2):
            small(k, 4).start()
        final[:, cols(t)] = moved[t]
        for k in range(1, 4):
            small_arrived(k, 6).wait_recv()
        for n in range(4):
            at = slice(n * width, n * width + width)
            out = jnp.zeros((32, width), f32)
            for x in range(4):
                out = out + jnp.dot(attx[x], wp[256 * x : 256 * x + 256, at], preferred_element_type=f32)
            mixed_ref[:, at] = out.astype(bf16)
        for k in range(1, 4):
            small_arrived(k, 4).wait_recv()
        o_ref[...] = final[...]

        def drain(ref, sem):
            remote(ref, ref, sem, arrive.at[0], me, left).wait_send()

        drain(slab.at[pl.ds(0, ranks - 1)], send_sem.at[0])
        drain(rows.at[pl.ds(0, 2)], send_sem.at[1])
        drain(rows.at[0], send_sem.at[2])
        drain(hid.at[pl.ds(0, 2)], send_sem.at[3])
        drain(hid.at[0], send_sem.at[4])
        drain(back.at[pl.ds(0, ranks - 1)], send_sem.at[27])
        for kind in (0, 1, 3, 4, 5, 6):
            for k in range(1, 4):
                small(k, kind).wait_send()
        for d in range(2):
            for step in range(1, 5):
                along_z(d, step).wait_send()
            lax.fori_loop(0, depth, lambda b, _, d=d: (along_y(d, b).wait_send(), 0)[1], 0)
            along_y2(d).wait_send()
        for i in range(4):
            across(i).wait_send()

    vmem = pl.BlockSpec(memory_space=pltpu.VMEM)
    hbm = pl.BlockSpec(memory_space=pl.ANY)
    return pl.pallas_call(
        kernel,
        out_shape=(jax.ShapeDtypeStruct((32, tokens.shape[1]), bf16), jax.ShapeDtypeStruct(tokens.shape, bf16)),
        in_specs=[hbm] * 17,
        out_specs=(vmem, vmem),
        scratch_shapes=[
            pltpu.VMEM(moe_gain.shape, moe_gain.dtype),
            pltpu.VMEM(routes.shape, routes.dtype),
            pltpu.VMEM(group_prob.shape, group_prob.dtype),
            pltpu.VMEM(expert_prob.shape, expert_prob.dtype),
            pltpu.VMEM(within.shape, within.dtype),
            pltpu.VMEM(starts.shape, starts.dtype),
            pltpu.VMEM(latent_gain.shape, latent_gain.dtype),
            pltpu.VMEM(tokens.shape, bf16),
            pltpu.VMEM(latent.shape, bf16),
            pltpu.VMEM(rope_key.shape, bf16),
            pltpu.VMEM(query.shape, bf16),
            pltpu.VMEM(tokens.shape, bf16),
            pltpu.VMEM((8, 128), f32),
            pltpu.VMEM((32, latent.shape[1] + 128), bf16),
            pltpu.VMEM((2, 4, 256, 256), bf16),
            pltpu.VMEM((128, 64), f32),
            pltpu.VMEM((4, 64, width), bf16),
            pltpu.VMEM((4, 8, 128), f32),
            pltpu.VMEM((ranks, 16, width), bf16),
            pltpu.VMEM((4, ranks, 16, width), bf16),
            pltpu.VMEM(w_gate.shape, bf16),
            pltpu.VMEM(w_up.shape, bf16),
            pltpu.VMEM((4, units, width), bf16),
            pltpu.VMEM((4, ranks, 16, units), bf16),
            pltpu.VMEM((ranks, 16, width), bf16),
            pltpu.VMEM((ranks, 16, width), bf16),
            pltpu.VMEM((4, 64, width), bf16),
            pltpu.VMEM(tokens.shape, bf16),
            pltpu.VMEM((256, ranks * 16), bf16),
            pltpu.VMEM((4, 32, latent.shape[1] + 128), bf16),
            pltpu.VMEM(key_up.shape, bf16),
            pltpu.VMEM(value_up.shape, bf16),
            pltpu.VMEM(out_proj.shape, bf16),
            pltpu.VMEM((8, depth, 544, 128), bf16),
            pltpu.VMEM((2, 1, 256), f32),
            pltpu.VMEM((2, 1, 256), f32),
            pltpu.VMEM((2, 128, 256), f32),
            pltpu.VMEM((4, 32, 256), bf16),
            pltpu.VMEM((4, 32, 256), bf16),
            pltpu.SemaphoreType.DMA((17,)),
            pltpu.SemaphoreType.DMA((1,)),
            pltpu.SemaphoreType.DMA((7, 4)),
            pltpu.SemaphoreType.DMA((ranks,)),
            pltpu.SemaphoreType.DMA((ranks,)),
            pltpu.SemaphoreType.DMA((4, 2, 8)),
            pltpu.SemaphoreType.DMA((28,)),
            pltpu.SemaphoreType.DMA((30,)),
            pltpu.SemaphoreType.DMA((30,)),
        ],
        compiler_params=pltpu.CompilerParams(
            collective_id=0, has_side_effects=True, vmem_limit_bytes=56 << 20
        ),
        cost_estimate=pl.CostEstimate(flops=5 * 10**9, bytes_accessed=3 * 10**7, transcendentals=0),
        name="exchange",
    )(
        tokens, moe_gain, routes, group_prob, expert_prob, within, starts, latent, rope_key, latent_gain,
        query, w_gate, w_up, w_down, key_up, value_up, out_proj,
    )


def body(
    query,
    latent,
    rope_key,
    latent_gain,
    key_up,
    value_up,
    out_proj,
    tokens,
    moe_gain,
    routes,
    group_prob,
    expert_prob,
    w_gate,
    w_up,
    w_down,
):
    rows = query.shape[0]
    within, starts = rotation(np.arange(rows)), rotation(np.arange(lax.axis_size("ep")) * rows)
    mixed, moe_out = exchange(
        tokens, moe_gain[None], routes.T, group_prob[None], expert_prob.T, within, starts, latent, rope_key, latent_gain[None],
        query, w_gate[0], w_up[0], w_down[0], key_up, value_up, out_proj,
    )
    return plain_copy(mixed, moe_out)


def solution(mesh):
    return jax.shard_map(
        body,
        mesh=mesh,
        in_specs=(
            P("ep", "tp"),
            P(("ep", "tp"), None),
            P(("ep", "tp"), None),
            P(),
            P(None, "tp"),
            P(None, "tp"),
            P(),
            P(("ep", "tp"), None),
            P(),
            P(("ep", "tp"), None),
            P(("ep", "tp")),
            P(("ep", "tp"), None),
            P("ep", None, "tp"),
            P("ep", None, "tp"),
            P("ep", "tp", None),
        ),
        out_specs=(P(("ep", "tp"), None), P(("ep", "tp"), None)),
        check_vma=False,
    )
```
